512 devices in a mesh: sp: 32 (over z, core), tp: 16 (over y, x).
Axes of the slice: x: 4, y: 4, z: 16, core: 2. Of those that a mesh axis runs over, the one named last changes fastest.
Arguments:
- residual: bfloat16 [4096, 2048], P('sp'), may hold values from -45 to 45
- query_a: bfloat16 [4096, 16, 128], P('sp', 'tp'), may hold values from -125 to 125
- keys_a: bfloat16 [4096, 16, 128], P('sp', 'tp'), may hold values from -8 to 8
- values_a: bfloat16 [4096, 16, 128], P('sp', 'tp'), may hold values from -6 to 6
- query_b: bfloat16 [4096, 16, 256], P('sp', 'tp'), may hold values from -125 to 125
- keys_b: bfloat16 [4096, 16, 256], P('sp', 'tp'), may hold values from -8 to 8
- values_b: bfloat16 [4096, 16, 256], P('sp', 'tp'), may hold values from -6 to 6
- lambda_a: float32 [16], P('tp'), may hold values from 0.3 to 0.8
- lambda_b: float32 [16], P('tp'), may hold values from 0.3 to 0.8
- gain_a: float32 [128], replicated, may hold values from 0.1 to 1.9
- gain_b: float32 [256], replicated, may hold values from 0.1 to 1.9
- proj_a: bfloat16 [2048, 2048], P('tp'), may hold values from -0.078125 to 0.078125
- proj_b: bfloat16 [4096, 2048], P('tp'), may hold values from -0.078125 to 0.078125
- norm_gain: float32 [2048], replicated, may hold values from 0.1 to 1.9
- routes: int32 [4096, 2], P('sp'), may hold values from 0 to 31, all different within a row; in each aligned block of 128 rows (0 to 127, 128 to 255, ...) at most 16 rows name the same one
- route_weight: float32 [4096, 2], P('sp'), may hold values from 0.2 to 2
- expert_gate: bfloat16 [32, 2048, 2048], P('sp', None, 'tp'), may hold values from -0.125 to 0.125
- expert_up: bfloat16 [32, 2048, 2048], P('sp', None, 'tp'), may hold values from -0.125 to 0.125
- expert_down: bfloat16 [32, 2048, 2048], P('sp', 'tp'), may hold values from -0.125 to 0.125
Outputs:
- layer_out: bfloat16 [4096, 2048], P('sp', 'tp')
The draws below stay inside these ranges and needn't reach their ends.
Inputs may be any that keep to these rules, and one draw needn't show every extreme that they name: `routes`: each row names 2 different experts; in each aligned block of 128 rows no expert is named more than 16 times, a bound that some block reaches.
All inputs are finite; a program needn't handle non-finite values.
Results may differ from the reference program's by a relative error of at most 0.013.
Values may be sent and summed in bfloat16 or wider, within the bound.
No kernel may reach another device: no remote copies, remote signals or barrier semaphores. Data moves between devices by JAX's collectives and lax.ppermute only.
A program may use at most 64 MiB of HBM per device.

```python
import math
import jax
import jax.numpy as jnp
import numpy as np
from jax import lax

D = 2048
HEADS = 16
DK_A = 64
DV_A = 128
DK_B = 128
DV_B = 256
DFF = 2048
SEG = 64
TOP = 2
TOK_DEV = 128
SEQ = 4096
EXPERTS = 32
CAP = 16
N_SP = 32
N_TP = 16


def query_key_pair(key, key_size, marker):
    base = jax.random.fold_in(key, marker)
    key_query, key_keys = jax.random.split(base, 2)
    shape = (SEQ, HEADS, 2, key_size)
    queries = jnp.clip(jax.random.normal(key_query, shape, jnp.float32), -6.0, 6.0) * 1.3
    keys_drawn = jnp.clip(jax.random.normal(key_keys, shape, jnp.float32), -6.0, 6.0) * 1.3
    return (queries.reshape(SEQ, HEADS, 2 * key_size), keys_drawn.reshape(SEQ, HEADS, 2 * key_size))


def draw_query_a(key, part):
    return query_key_pair(key, DK_A, 11)[0].astype(jnp.bfloat16)


def draw_keys_a(key, part):
    return query_key_pair(key, DK_A, 11)[1].astype(jnp.bfloat16)


def draw_query_b(key, part):
    return query_key_pair(key, DK_B, 23)[0].astype(jnp.bfloat16)


def draw_keys_b(key, part):
    return query_key_pair(key, DK_B, 23)[1].astype(jnp.bfloat16)


def draw_residual(key, part):
    base = jax.random.fold_in(key, 37)
    key_values = jax.random.fold_in(base, 0)
    column = jnp.exp(math.log(0.35) + math.log(9.0) * jnp.arange(D, dtype=jnp.float32) / (D - 1))
    values = jnp.clip(jax.random.normal(key_values, (SEQ, D), jnp.float32), -6.0, 6.0) * column[None, :]
    return values.astype(jnp.bfloat16)


def block_scale(key, shape, shards, smallest, top_value):
    loudness, own = 1.0, jax.random.fold_in(key, 6)
    for axis_at, parts in shards:
        steps = jnp.exp(jax.random.uniform(jax.random.fold_in(own, axis_at), (parts,), jnp.float32, smallest / len(shards), top_value / len(shards)))
        loudness = loudness * jnp.repeat(steps, shape[axis_at] // parts).reshape([-1 if axis == axis_at else 1 for axis in range(len(shape))])
    return loudness


def shared_out(own_key, own, number, rows, number_of, top, reach, lean):
    sequence = jax.random.permutation(own_key, number_of)
    packed, usual = shares(number_of, rows * top, reach, lean, True), shares(number_of, rows * top, reach, lean, False)
    places = jnp.arange(number_of)

    def named(sizes, offset_by):
        used = int((sizes > 0).sum())
        fixed = max(1, used // 4)
        passed = fixed + (places - fixed + offset_by * (used - fixed)) % max(1, number_of - fixed)
        return jnp.zeros((number_of,), jnp.int32).at[sequence[jnp.where(places < fixed, places, passed)]].set(jnp.asarray(sizes, jnp.int32))

    sizes = jnp.where(number % 4 == 0, named(packed, number // 4), named(usual, number - number // 4 - 1))
    mixed = jax.random.permutation(jax.random.fold_in(own, 3), number_of)
    source_of, receiver = mixed[0:number_of // 2 * 2:2], mixed[1:number_of // 2 * 2:2]
    slack = jnp.minimum(sizes[source_of] - 1, reach - sizes[receiver]) // 2
    slack = jnp.where((source_of == sequence[0]) | (receiver == sequence[0]) | (sizes[receiver] == 0), 0, jnp.maximum(slack, 0))
    passed = jax.random.randint(jax.random.fold_in(own, 4), (number_of // 2,), 0, 1 << 20) % (slack + 1)
    sizes = sizes.at[source_of].add(-passed).at[receiver].add(passed)
    labels = jnp.searchsorted(jnp.cumsum(sizes), jnp.arange(rows * top), side="right").astype(jnp.int32)
    table = labels.reshape(top, rows).T
    table = table[jax.random.permutation(jax.random.fold_in(own, 1), rows)]
    offset_by = jax.random.randint(jax.random.fold_in(own, 2), (rows, 1), 0, top)
    return jnp.take_along_axis(table, (jnp.arange(top)[None, :] + offset_by) % top, axis=1)


def shares(number_of, total, limit, skew, full):
    portions = [(1 << 20) // math.isqrt(standing ** skew) + 1 for standing in range(1, number_of + 1)]
    largest = limit if full else min(limit, max(-(-total // number_of), total * portions[0] // sum(portions)))
    least = 1 if total - largest >= number_of - 1 else 0
    given, spare = [largest] + [least] * (number_of - 1), total - largest - least * (number_of - 1)
    while spare > 0:
        free = [i for i in range(1, number_of) if given[i] < largest] or [i for i in range(1, number_of) if given[i] < limit]
        pool, left = sum([portions[i] for i in free]), spare
        for i in free:
            addition = min(limit - given[i], max(1, left * portions[i] // pool), spare)
            given[i] = given[i] + addition
            spare = spare - addition
    return np.array(given)


def normal_values(stream_key, extent, scale, reach, cuts=(), kind=jnp.bfloat16):
    values = scale * jax.random.normal(stream_key, extent, jnp.float32)
    if cuts:
        values = values * block_scale(stream_key, extent, cuts, -0.22, 0.18)
    return jnp.clip(values, -reach, reach).astype(kind)


def setup_inputs(seed: int = 0) -> dict:
    keys = jax.random.split(jax.random.key(seed), 20)
    residual = draw_residual(jax.random.fold_in(keys[19], 71), 0)
    query_a = draw_query_a(jax.random.fold_in(keys[19], 71), 0)
    keys_a = draw_keys_a(jax.random.fold_in(keys[19], 71), 0)
    values_a = normal_values(keys[3], (SEQ, HEADS, DV_A), 1.0, 6.0, ((0, 32), (1, 16)))
    query_b = draw_query_b(jax.random.fold_in(keys[19], 71), 0)
    keys_b = draw_keys_b(jax.random.fold_in(keys[19], 71), 0)
    values_b = normal_values(keys[6], (SEQ, HEADS, DV_B), 1.0, 6.0, ((0, 32), (1, 16)))
    lambda_a = jnp.clip(0.3 + 0.5 * jax.random.uniform(keys[7], (HEADS,), jnp.float32) ** block_scale(keys[7], (HEADS,), ((0, 16),), -0.2, 0.2), 0.3, 0.8)
    lambda_b = jnp.clip(0.3 + 0.5 * jax.random.uniform(keys[8], (HEADS,), jnp.float32) ** block_scale(keys[8], (HEADS,), ((0, 16),), -0.2, 0.2), 0.3, 0.8)
    gain_a = jnp.clip(1.0 + 0.18 * jax.random.normal(keys[9], (DV_A,), jnp.float32), 0.1, 1.9)
    gain_b = jnp.clip(1.0 + 0.18 * jax.random.normal(keys[10], (DV_B,), jnp.float32), 0.1, 1.9)
    proj_a = normal_values(keys[11], (HEADS * DV_A, D), (HEADS * (DV_A + DV_B)) ** -0.5, 0.078125, ((0, 16),))
    proj_b = normal_values(keys[12], (HEADS * DV_B, D), (HEADS * (DV_A + DV_B)) ** -0.5, 0.078125, ((0, 16),))
    norm_gain = jnp.clip(1.0 + 0.18 * jax.random.normal(keys[13], (D,), jnp.float32), 0.1, 1.9)
    routes_keys = jax.random.split(jax.random.fold_in(keys[14], 1), SEQ // TOK_DEV)
    routes_turns = jax.random.permutation(jax.random.fold_in(keys[14], 3), SEQ // TOK_DEV)
    routes = jax.vmap(lambda own, number: shared_out(jax.random.fold_in(keys[14], 2), own, number, TOK_DEV, EXPERTS, TOP, CAP, 1))(routes_keys, routes_turns).reshape((SEQ, TOP))
    route_weight = jnp.clip(jnp.exp(math.log(2.0) - 2.3025851 * jax.random.uniform(keys[15], (SEQ, TOP), jnp.float32) ** block_scale(keys[15], (SEQ, TOP), ((0, 32),), -0.2, 0.2)), 0.2, 2.0)
    expert_gate = normal_values(keys[16], (EXPERTS, D, DFF), D ** -0.5, 0.125, ((0, 32), (2, 16)))
    expert_up = normal_values(keys[17], (EXPERTS, D, DFF), D ** -0.5, 0.125, ((0, 32), (2, 16)))
    expert_down = normal_values(keys[18], (EXPERTS, DFF, D), DFF ** -0.5, 0.125, ((0, 32), (1, 16)))
    return dict(residual=residual, query_a=query_a, keys_a=keys_a, values_a=values_a, query_b=query_b, keys_b=keys_b, values_b=values_b, lambda_a=lambda_a, lambda_b=lambda_b, gain_a=gain_a, gain_b=gain_b, proj_a=proj_a, proj_b=proj_b, norm_gain=norm_gain, routes=routes, route_weight=route_weight, expert_gate=expert_gate, expert_up=expert_up, expert_down=expert_down)


EPS = 1e-06

def attend_group(queries, keys_all, values_all, mixing, head_gain, key_size):
    seq_rows = queries.shape[0]
    query_block = 512 if seq_rows % 512 == 0 else seq_rows
    positions = jnp.arange(seq_rows, dtype=jnp.int32)
    segment = positions // SEG
    factor = key_size ** (-0.5)
    keys_wide = keys_all.astype(jnp.float32)
    values_wide = values_all.astype(jnp.float32)

    def one_block(first_row):
        block_queries = lax.dynamic_slice_in_dim(queries, first_row, query_block, 0).astype(jnp.float32)
        block_segment = lax.dynamic_slice_in_dim(segment, first_row, query_block, 0)
        visible = block_segment[:, None] >= segment[None, :]

        def softmax_map(map_queries, map_keys):
            raw_scores = jnp.einsum('qhd,khd->hqk', map_queries, map_keys) * factor
            raw_scores = jnp.where(visible[None], raw_scores, -jnp.inf)
            largest = lax.optimization_barrier(jnp.max(raw_scores, axis=-1, keepdims=True))
            expo = jnp.exp(raw_scores - largest)
            return expo / lax.optimization_barrier(jnp.sum(expo, axis=-1, keepdims=True))
        first_probs = softmax_map(block_queries[..., :key_size], keys_wide[..., :key_size])
        second_probs = softmax_map(block_queries[..., key_size:], keys_wide[..., key_size:])
        weights = (first_probs - mixing[:, None, None] * second_probs).astype(jnp.bfloat16)
        mixed = jnp.einsum('hqk,khe->qhe', weights.astype(jnp.float32), values_wide)
        mean_sq = lax.optimization_barrier(jnp.mean(mixed * mixed, axis=-1, keepdims=True))
        return (mixed * lax.rsqrt(mean_sq + EPS) * head_gain).astype(jnp.bfloat16)
    starts = jnp.arange(seq_rows // query_block, dtype=jnp.int32) * query_block
    blocks = lax.map(one_block, starts)
    return blocks.reshape(seq_rows, -1)

def reference(residual, query_a, keys_a, values_a, query_b, keys_b, values_b, lambda_a, lambda_b, gain_a, gain_b, proj_a, proj_b, norm_gain, routes, route_weight, expert_gate, expert_up, expert_down):
    heads_a = attend_group(query_a, keys_a, values_a, lambda_a, gain_a, DK_A)
    heads_b = attend_group(query_b, keys_b, values_b, lambda_b, gain_b, DK_B)
    branch = jnp.dot(heads_a, proj_a, preferred_element_type=jnp.float32) + jnp.dot(heads_b, proj_b, preferred_element_type=jnp.float32)
    stream = (residual.astype(jnp.float32) + branch).astype(jnp.bfloat16)
    stream_wide = stream.astype(jnp.float32)
    mean_sq = lax.optimization_barrier(jnp.mean(stream_wide * stream_wide, axis=-1, keepdims=True))
    normed = (stream_wide * lax.rsqrt(mean_sq + EPS) * norm_gain).astype(jnp.bfloat16)
    assign = routes.reshape(N_SP, TOK_DEV * TOP)
    onehot = (assign[..., None] == jnp.arange(EXPERTS, dtype=jnp.int32)).astype(jnp.int32)
    earlier = jnp.cumsum(onehot, axis=1) - onehot
    slot_index = lax.optimization_barrier(jnp.sum(earlier * onehot, axis=-1))
    block_ids = jnp.arange(N_SP, dtype=jnp.int32)[:, None]
    target = ((block_ids * EXPERTS + assign) * CAP + slot_index).reshape(-1).astype(jnp.int32)
    token_ids = (jnp.arange(SEQ * TOP, dtype=jnp.int32) // TOP).astype(jnp.int32)
    buffer = jnp.zeros((N_SP * EXPERTS * CAP, D), jnp.bfloat16).at[target].set(normed[token_ids])
    grouped = buffer.reshape(N_SP, EXPERTS, CAP, D).transpose(1, 0, 2, 3).reshape(EXPERTS, N_SP * CAP, D)

    def one_expert(operands):
        rows, weight_gate, weight_up, weight_down = operands
        gate_val = jnp.dot(rows, weight_gate, preferred_element_type=jnp.float32)
        up_val = jnp.dot(rows, weight_up, preferred_element_type=jnp.float32)
        hidden = (jax.nn.silu(gate_val) * up_val).astype(jnp.bfloat16)
        hidden_blocks = hidden.reshape(rows.shape[0], N_TP, DFF // N_TP).astype(jnp.float32)
        down_blocks = weight_down.reshape(N_TP, DFF // N_TP, D).astype(jnp.float32)
        pieces = jnp.einsum('rjf,jfd->jrd', hidden_blocks, down_blocks)
        rounded = lax.optimization_barrier(pieces.astype(jnp.bfloat16))
        return lax.optimization_barrier(jnp.sum(rounded.astype(jnp.float32), axis=0)).astype(jnp.bfloat16)
    outputs = lax.map(one_expert, (grouped, expert_gate, expert_up, expert_down))
    flat_out = outputs.reshape(EXPERTS, N_SP, CAP, D).transpose(1, 0, 2, 3).reshape(-1, D)
    picked = flat_out[target].astype(jnp.float32).reshape(SEQ, TOP, D)
    gates = route_weight / lax.optimization_barrier(jnp.sum(route_weight, axis=-1, keepdims=True))
    experts_sum = lax.optimization_barrier(jnp.sum(gates[..., None] * picked, axis=1))
    return (stream_wide + experts_sum).astype(jnp.bfloat16)
```

```python
import jax
import jax.numpy as jnp
from jax import lax
from jax.sharding import PartitionSpec as P

DK_A = 64
DK_B = 128
SEG = 64
TOP = 2
GROUP = 4


EPS = 1e-06


def side_by_side(arrays, axis, dim, along):
    ends, at = ([], 0)
    for a in arrays[:-1]:
        at += a.shape[along]
        ends.append(at)
    both = jnp.concatenate(arrays, axis=along)
    return tuple(jnp.split(lax.all_gather(both, axis, axis=dim, tiled=True), ends, axis=along))


def split_up(value, dim, count):
    dims = value.shape
    pieces = value.reshape(*dims[:dim], count, dims[dim] // count, *dims[dim + 1 :])
    return jnp.moveaxis(pieces, dim, 0)


def summed_on_arrival(value, axis, dim):
    pieces = split_up(value, dim, lax.axis_size(axis))
    arrived = lax.all_to_all(pieces, axis, split_axis=0, concat_axis=0, tiled=True)
    return arrived.astype(jnp.float32).sum(axis=0)


def in_order(pieces, dim):
    pieces = jnp.moveaxis(pieces, 0, dim)
    dims = pieces.shape
    return pieces.reshape(*dims[:dim], dims[dim] * dims[dim + 1], *dims[dim + 2 :])


def over_lines(value, count, dim):
    width = count // GROUP
    blocks = [value]
    for step in range(1, GROUP):
        pairs = [(i, (i + step * width) % count) for i in range(count)]
        blocks.append(lax.ppermute(value, "tp", pairs))
    return jnp.concatenate(blocks, axis=dim)


def attend_local(queries, keys_all, values_all, mixing, head_gain, key_size, offset, block_rows):
    tok_rows = queries.shape[0]
    heads_local = queries.shape[1]
    positions = offset + jnp.arange(tok_rows, dtype=jnp.int32)
    query_seg = positions // SEG
    factor = key_size ** (-0.5)
    needed = (offset + tok_rows + block_rows - 1) // block_rows
    first_query = queries[..., :key_size]
    second_query = queries[..., key_size:]

    def block_scores(start, map_query, block_keys):
        raw_scores = (
            jnp.einsum("qhd,khd->hqk", map_query, block_keys, preferred_element_type=jnp.float32)
            * factor
        )
        key_seg = (start + jnp.arange(block_rows, dtype=jnp.int32)) // SEG
        visible = query_seg[:, None] >= key_seg[None, :]
        return jnp.where(visible[None], raw_scores, -jnp.inf)

    def both_scores(block_index):
        start = block_index * block_rows
        block_keys = lax.dynamic_slice_in_dim(keys_all, start, block_rows, 0)
        first_scores = block_scores(start, first_query, block_keys[..., :key_size])
        second_scores = block_scores(start, second_query, block_keys[..., key_size:])
        return (start, first_scores, second_scores)

    def update(old_max, old_sum, scores):
        new_max = jnp.maximum(old_max, jnp.max(scores, axis=-1, keepdims=True))
        new_sum = old_sum * jnp.exp(old_max - new_max) + jnp.sum(
            jnp.exp(scores - new_max), axis=-1, keepdims=True
        )
        return (new_max, new_sum)

    def statistics(block_index, running):
        first_max, first_sum, second_max, second_sum = running
        start, first_scores, second_scores = both_scores(block_index)
        first_max, first_sum = update(first_max, first_sum, first_scores)
        second_max, second_sum = update(second_max, second_sum, second_scores)
        return (first_max, first_sum, second_max, second_sum)

    start_max = jnp.full((heads_local, tok_rows, 1), -jnp.inf, jnp.float32)
    start_sum = jnp.zeros((heads_local, tok_rows, 1), jnp.float32)
    first_max, first_sum, second_max, second_sum = lax.fori_loop(
        0, needed, statistics, (start_max, start_sum, start_max, start_sum)
    )
    mix_col = mixing[:, None, None]

    def accumulate(block_index, summed_rows):
        start, first_scores, second_scores = both_scores(block_index)
        first_probs = jnp.exp(first_scores - first_max) / first_sum
        second_probs = jnp.exp(second_scores - second_max) / second_sum
        block_weights = (first_probs - mix_col * second_probs).astype(jnp.bfloat16)
        block_values = lax.dynamic_slice_in_dim(values_all, start, block_rows, 0)
        return summed_rows + jnp.einsum(
            "hqk,khe->qhe", block_weights, block_values, preferred_element_type=jnp.float32
        )

    mixed = lax.fori_loop(
        0, needed, accumulate, jnp.zeros((tok_rows, heads_local, values_all.shape[2]), jnp.float32)
    )
    mean_sq = jnp.mean(mixed * mixed, axis=-1, keepdims=True)
    return (mixed * lax.rsqrt(mean_sq + EPS) * head_gain).astype(jnp.bfloat16)


def local(
    residual,
    query_a,
    keys_a,
    values_a,
    query_b,
    keys_b,
    values_b,
    lambda_a,
    lambda_b,
    gain_a,
    gain_b,
    proj_a,
    proj_b,
    norm_gain,
    routes,
    route_weight,
    expert_gate,
    expert_up,
    expert_down,
):
    tok_rows = residual.shape[0]
    model_width = residual.shape[1]
    seq_devices = lax.axis_size("sp")
    head_devices = lax.axis_size("tp")
    head_index = lax.axis_index("tp")
    offset = lax.axis_index("sp") * tok_rows
    every_keys_a, every_values_a, every_keys_b, every_values_b = side_by_side(
        (keys_a, values_a, keys_b, values_b), "sp", 0, 2
    )
    wide_gate = over_lines(expert_gate[0], head_devices, 1)
    wide_up = over_lines(expert_up[0], head_devices, 1)
    wide_down = over_lines(expert_down[0], head_devices, 0)
    block_rows = 512
    heads_a = attend_local(
        query_a, every_keys_a, every_values_a, lambda_a, gain_a, DK_A, offset, block_rows
    )
    heads_b = attend_local(
        query_b, every_keys_b, every_values_b, lambda_b, gain_b, DK_B, offset, block_rows
    )
    partial_branch = jnp.dot(
        heads_a.reshape(tok_rows, -1), proj_a, preferred_element_type=jnp.float32
    )
    partial_branch = partial_branch + jnp.dot(
        heads_b.reshape(tok_rows, -1), proj_b, preferred_element_type=jnp.float32
    )
    columns = model_width // head_devices
    col_start = head_index * columns
    summed_cols = summed_on_arrival(partial_branch.astype(jnp.bfloat16), "tp", 1)
    residual_cols = lax.dynamic_slice_in_dim(residual, col_start, columns, 1)
    stream_cols = (residual_cols.astype(jnp.float32) + summed_cols).astype(jnp.bfloat16)
    slot_count = 2 * tok_rows * TOP // seq_devices
    assign = routes.reshape(-1)
    onehot = (assign[:, None] == jnp.arange(seq_devices, dtype=jnp.int32)[None, :]).astype(
        jnp.int32
    )
    earlier = jnp.cumsum(onehot, axis=0) - onehot
    slot_index = jnp.sum(earlier * onehot, axis=1)
    target = assign * slot_count + slot_index
    placed = (
        target[:, None] == jnp.arange(seq_devices * slot_count, dtype=jnp.int32)[None, :]
    ).reshape(tok_rows, TOP, -1)
    select = jnp.sum(placed.astype(jnp.bfloat16), axis=1)
    gates = route_weight / jnp.sum(route_weight, axis=1, keepdims=True)
    combine = jnp.sum(placed.astype(jnp.float32) * gates[:, :, None], axis=1)
    send_rows = jnp.einsum(
        "ts,td->sd", select, stream_cols, preferred_element_type=jnp.float32
    ).astype(jnp.bfloat16)
    send_rows = send_rows.reshape(seq_devices, slot_count, columns)
    routed = lax.all_to_all(send_rows, "sp", split_axis=0, concat_axis=0, tiled=True)
    group_rows = seq_devices * slot_count // GROUP
    grouped = routed.reshape(GROUP, 1, group_rows, columns)
    copies = jnp.broadcast_to(grouped, (GROUP, head_devices // GROUP, group_rows, columns))
    arrived = lax.all_to_all(
        copies.reshape(head_devices, group_rows, columns),
        "tp",
        split_axis=0,
        concat_axis=0,
        tiled=True,
    )
    rows = in_order(arrived, 1).astype(jnp.float32)
    squares = jnp.sum(rows * rows, axis=1, keepdims=True)
    normed = (rows * lax.rsqrt(squares / model_width + EPS) * norm_gain).astype(jnp.bfloat16)
    gate_val = jnp.dot(normed, wide_gate, preferred_element_type=jnp.float32)
    up_val = jnp.dot(normed, wide_up, preferred_element_type=jnp.float32)
    hidden = (jax.nn.silu(gate_val) * up_val).astype(jnp.bfloat16)
    down_part = jnp.dot(hidden, wide_down, preferred_element_type=jnp.float32)
    parts = split_up(down_part.astype(jnp.bfloat16), 1, head_devices)
    parts = lax.all_to_all(parts, "tp", split_axis=0, concat_axis=0, tiled=True)
    results = (
        parts.reshape(GROUP, head_devices // GROUP, group_rows, columns)
        .astype(jnp.float32)
        .sum(axis=1)
        .astype(jnp.bfloat16)
        .reshape(seq_devices, slot_count, columns)
    )
    returned = lax.all_to_all(results, "sp", split_axis=0, concat_axis=0, tiled=True)
    returned_flat = returned.reshape(seq_devices * slot_count, columns).astype(jnp.float32)
    experts_sum = jnp.dot(combine, returned_flat, precision=lax.Precision.HIGHEST)
    return (stream_cols.astype(jnp.float32) + experts_sum).astype(jnp.bfloat16)


def solution(mesh):
    placed = (
        P("sp", None),
        P("sp", "tp", None),
        P("sp", "tp", None),
        P("sp", "tp", None),
        P("sp", "tp", None),
        P("sp", "tp", None),
        P("sp", "tp", None),
        P("tp"),
        P("tp"),
        P(),
        P(),
        P("tp", None),
        P("tp", None),
        P(),
        P("sp", None),
        P("sp", None),
        P("sp", None, "tp"),
        P("sp", None, "tp"),
        P("sp", "tp", None),
    )
    return jax.shard_map(
        local, mesh=mesh, in_specs=placed, out_specs=P("sp", "tp"), check_vma=False
    )
```

```python
import functools

import jax
import jax.numpy as jnp
from jax import lax
from jax.experimental import pallas as pl
from jax.experimental.pallas import tpu as pltpu
from jax.sharding import PartitionSpec as P

DK_A = 64
DK_B = 128
SEG = 64
TOP = 2
LINE = 4
EPS = 1e-06
LOW = -1e30


VMEM = pl.BlockSpec(memory_space=pltpu.VMEM)
SMEM = pl.BlockSpec(memory_space=pltpu.SMEM)

MAPS = (
    (slice(0, 128), slice(0, 128), slice(128, 256), slice(0, 128), DK_A**-0.5),
    (slice(128, 256), slice(0, 128), slice(128, 256), slice(128, 256), DK_A**-0.5),
    (slice(256, 384), slice(256, 384), slice(512, 768), slice(256, 512), DK_B**-0.5),
    (slice(384, 512), slice(384, 512), slice(512, 768), slice(512, 768), DK_B**-0.5),
)
SUMS = 768
STATE = SUMS + 8


def absorb(first, blocks, flag_ref, q_ref, *refs):
    kv_refs = refs[:blocks]
    olds = None if first else refs[blocks : blocks + 2]
    outs = refs[-2:]
    half = outs[0].shape[1]

    def both(refs, rows):
        return jnp.concatenate([r[rows, :] for r in refs], axis=1)

    def keep(rows, value):
        outs[0][rows, :] = value[:, :half]
        outs[1][rows, :] = value[:, half:]

    def work():
        for index, (q_cols, k_cols, v_cols, rows, factor) in enumerate(MAPS):
            keys = jnp.concatenate([r[:, k_cols] for r in kv_refs], axis=0)
            values = jnp.concatenate([r[:, v_cols] for r in kv_refs], axis=0)
            scores = (
                lax.dot_general(
                    keys,
                    q_ref[:, q_cols],
                    (((1,), (1,)), ((), ())),
                    preferred_element_type=jnp.float32,
                )
                * factor
            )
            at_max = slice(SUMS + index, SUMS + index + 1)
            at_sum = slice(SUMS + 4 + index, SUMS + 5 + index)
            if first:
                key_seg = lax.broadcasted_iota(jnp.int32, scores.shape, 0) // SEG
                column = lax.broadcasted_iota(jnp.int32, scores.shape, 1)
                query_seg = jnp.where(
                    column < half, column // SEG, (column - half) // SEG + flag_ref[0]
                )
                visible = key_seg <= query_seg
                scores = jnp.where(visible, scores, LOW)
                new_max = jnp.max(scores, axis=0, keepdims=True)
                expo = jnp.where(visible, jnp.exp(scores - new_max), 0.0)
            else:
                old_max = both(olds, at_max)
                new_max = jnp.maximum(old_max, jnp.max(scores, axis=0, keepdims=True))
                expo = jnp.exp(scores - new_max)
            total = jnp.sum(expo, axis=0, keepdims=True)
            summed = lax.dot_general(
                values,
                expo.astype(jnp.bfloat16),
                (((0,), (0,)), ((), ())),
                preferred_element_type=jnp.float32,
            )
            if not first:
                shrink = jnp.exp(old_max - new_max)
                total = total + both(olds, at_sum) * shrink
                summed = summed + both(olds, rows) * shrink
            keep(rows, summed)
            keep(at_max, new_max)
            keep(at_sum, total)

    if first:
        work()
    else:
        pl.when(flag_ref[0] > 0)(work)

        @pl.when(flag_ref[0] <= 0)
        def _():
            outs[0][...] = olds[0][...]
            outs[1][...] = olds[1][...]


def absorbed(flag, queries, kvs, olds):
    half = queries.shape[0] // 2
    shape = jax.ShapeDtypeStruct((STATE, half), jnp.float32)
    keys = len(kvs) * kvs[0].shape[0]
    return pl.pallas_call(
        functools.partial(absorb, olds is None, len(kvs)),
        out_shape=(shape, shape),
        in_specs=[SMEM] + [VMEM] * (1 + len(kvs) + (0 if olds is None else 2)),
        out_specs=(VMEM, VMEM),
        cost_estimate=pl.CostEstimate(
            flops=2 * 2 * half * keys * (512 + SUMS), bytes_accessed=0, transcendentals=0
        ),
        name="absorb",
    )(flag, queries, *kvs, *(olds or ()))


def finish(mix_ref, own_ref, got_ref, gain_a_ref, gain_b_ref, proj_a_ref, proj_b_ref, out_ref):
    def merged(index):
        at_max = slice(SUMS + index, SUMS + index + 1)
        at_sum = slice(SUMS + 4 + index, SUMS + 5 + index)
        rows = MAPS[index][3]
        own_max, got_max = own_ref[at_max, :], got_ref[at_max, :]
        new_max = jnp.maximum(own_max, got_max)
        own_w, got_w = jnp.exp(own_max - new_max), jnp.exp(got_max - new_max)
        total = own_ref[at_sum, :] * own_w + got_ref[at_sum, :] * got_w
        return own_ref[rows, :] * (own_w / total) + got_ref[rows, :] * (got_w / total)

    def head(index, mixing, gain_ref):
        mixed = merged(index) - mixing * merged(index + 1)
        mean_sq = jnp.mean(mixed * mixed, axis=0, keepdims=True)
        return (mixed * lax.rsqrt(mean_sq + EPS) * gain_ref[...]).astype(jnp.bfloat16)

    heads_a = head(0, mix_ref[0], gain_a_ref)
    heads_b = head(2, mix_ref[1], gain_b_ref)
    width = out_ref.shape[2]
    across = (((0,), (0,)), ((), ()))
    step = 4
    for piece in range(0, out_ref.shape[0], step):
        cols = slice(piece * width, (piece + step) * width)
        branch = lax.dot_general(
            heads_a, proj_a_ref[:, cols], across, preferred_element_type=jnp.float32
        ) + lax.dot_general(
            heads_b, proj_b_ref[:, cols], across, preferred_element_type=jnp.float32
        )
        for i in range(step):
            out_ref[piece + i] = branch[:, i * width : (i + 1) * width].astype(jnp.bfloat16)


def experts(rows_ref, gain_ref, own_ref, low_ref, high_ref, far_low_ref, far_high_ref, out_ref):
    parts, _, width = rows_ref.shape
    model_width = parts * width
    rows = jnp.concatenate([rows_ref[i] for i in range(parts)], axis=1).astype(jnp.float32)
    mean_sq = jnp.sum(rows * rows, axis=1, keepdims=True) / model_width
    normed = (rows * lax.rsqrt(mean_sq + EPS) * gain_ref[...]).astype(jnp.bfloat16)
    cut = far_low_ref.shape[0]

    def act(both):
        gate, up = both[:, :width], both[:, width:]
        return (gate / (1.0 + jnp.exp(-gate)) * up).astype(jnp.bfloat16)

    def dot(a, b):
        return jnp.dot(a, b, preferred_element_type=jnp.float32)

    whole = (own_ref, low_ref, high_ref)
    hidden = [act(dot(normed, ref[:model_width, :])) for ref in whole]
    far = dot(normed[:, :cut], far_low_ref[...]) + dot(
        normed[:, cut:], far_high_ref[: model_width - cut, :]
    )
    hidden.append(act(far))
    for j in range(parts // 2):
        start = model_width + j * width
        down = dot(hidden[3], far_high_ref[start - cut : start - cut + width, :])
        for i, ref in enumerate(whole):
            down = down + dot(hidden[i], ref[start : start + width, :])
        out_ref[2 * j] = down[:, :width].astype(jnp.bfloat16)
        out_ref[2 * j + 1] = down[:, width:].astype(jnp.bfloat16)


def summed_on_arrival(pieces, axis):
    arrived = lax.all_to_all(pieces, axis, split_axis=0, concat_axis=0, tiled=True)
    return arrived.astype(jnp.float32)


def local(
    residual,
    query_a,
    keys_a,
    values_a,
    query_b,
    keys_b,
    values_b,
    lambda_a,
    lambda_b,
    gain_a,
    gain_b,
    proj_a,
    proj_b,
    norm_gain,
    routes,
    route_weight,
    expert_gate,
    expert_up,
    expert_down,
):
    tok_rows = residual.shape[0]
    model_width = residual.shape[1]
    seq_devices = lax.axis_size("sp")
    head_devices = lax.axis_size("tp")
    head_index = lax.axis_index("tp")
    seq_index = lax.axis_index("sp")
    columns = model_width // head_devices

    chips = seq_devices // 2
    chip, core = seq_index // 2, seq_index % 2
    partner = [(i, i ^ 1) for i in range(seq_devices)]
    onward = [(2 * i, 2 * ((i + 1) % chips)) for i in range(chips)]
    onward += [(2 * i + 1, 2 * ((i - 1) % chips) + 1) for i in range(chips)]

    own_kv = jnp.concatenate([keys_a[:, 0], values_a[:, 0], keys_b[:, 0], values_b[:, 0]], axis=1)
    own_q = jnp.concatenate([query_a[:, 0], query_b[:, 0]], axis=1)
    got = lax.ppermute(jnp.concatenate([own_q, own_kv], axis=1), "sp", partner)
    got_kv = got[:, own_q.shape[1] :]
    q_rows = jnp.concatenate([own_q, got[:, : own_q.shape[1]]], axis=0)
    lane = jnp.arange(2 * DK_A)[None, :]
    q_first = jnp.where(lane < DK_A, q_rows[:, : 2 * DK_A], 0)
    q_second = jnp.where(lane < DK_A, 0, q_rows[:, : 2 * DK_A])
    queries = jnp.concatenate([q_first, q_second, q_rows[:, 2 * DK_A :]], axis=1)

    lines = head_devices // LINE
    width = expert_gate.shape[2]
    gate_up = jnp.concatenate([expert_gate[0], expert_up[0]], axis=1)
    down = expert_down[0].reshape(width, -1, 2 * width).transpose(1, 0, 2).reshape(-1, 2 * width)
    packed = jnp.concatenate([gate_up, down], axis=0)
    cut = packed.shape[0] // 2
    ahead = [(i, (i + lines) % head_devices) for i in range(head_devices)]
    back = [(i, (i - lines) % head_devices) for i in range(head_devices)]
    low = lax.ppermute(packed, "tp", ahead)
    high = lax.ppermute(packed, "tp", back)
    far_low = lax.ppermute(low[:cut], "tp", ahead)
    far_high = lax.ppermute(high[cut:], "tp", back)

    segments = tok_rows // SEG
    later = jnp.where(core == 0, segments, -segments).astype(jnp.int32).reshape(1)
    state = absorbed(later, queries, (own_kv,), None)
    mine, theirs = own_kv, got_kv
    for step in range(1, chips // 2 + 1):
        source = jnp.where(core == 0, chip - step, chip + step) % chips
        seen = (source < chip).astype(jnp.int32).reshape(1)
        mine = lax.ppermute(mine, "sp", onward)
        if step < chips // 2:
            theirs = lax.ppermute(theirs, "sp", onward)
            state = absorbed(seen, queries, (mine, theirs), state)
        else:
            state = absorbed(seen, queries, (mine,), state)
    got_state = lax.ppermute(state[1], "sp", partner)
    pieces = pl.pallas_call(
        finish,
        out_shape=jax.ShapeDtypeStruct((head_devices, tok_rows, columns), jnp.bfloat16),
        in_specs=[SMEM] + [VMEM] * 6,
        out_specs=VMEM,
        name="finish",
    )(
        jnp.concatenate([lambda_a, lambda_b]),
        state[0],
        got_state,
        gain_a[:, None],
        gain_b[:, None],
        proj_a,
        proj_b,
    )

    col_start = head_index * columns
    summed_cols = summed_on_arrival(pieces, "tp").sum(axis=0)
    residual_cols = lax.dynamic_slice_in_dim(residual, col_start, columns, 1)
    stream_cols = (residual_cols.astype(jnp.float32) + summed_cols).astype(jnp.bfloat16)
    slot_count = 2 * tok_rows * TOP // seq_devices
    assign = routes.reshape(-1)
    onehot = (assign[:, None] == jnp.arange(seq_devices, dtype=jnp.int32)[None, :]).astype(
        jnp.int32
    )
    earlier = jnp.cumsum(onehot, axis=0) - onehot
    slot_index = jnp.sum(earlier * onehot, axis=1)
    target = assign * slot_count + slot_index
    placed = (
        target[:, None] == jnp.arange(seq_devices * slot_count, dtype=jnp.int32)[None, :]
    ).reshape(tok_rows, TOP, -1)
    select = jnp.sum(placed.astype(jnp.bfloat16), axis=1)
    gates = route_weight / jnp.sum(route_weight, axis=1, keepdims=True)
    combine = jnp.sum(placed.astype(jnp.float32) * gates[:, :, None], axis=1)
    send_rows = jnp.einsum(
        "ts,td->sd", select, stream_cols, preferred_element_type=jnp.float32
    ).astype(jnp.bfloat16)
    send_rows = send_rows.reshape(seq_devices, slot_count, columns)
    routed = lax.all_to_all(send_rows, "sp", split_axis=0, concat_axis=0, tiled=True)
    group_rows = seq_devices * slot_count // LINE
    grouped = routed.reshape(LINE, 1, group_rows, columns)
    copies = jnp.broadcast_to(grouped, (LINE, lines, group_rows, columns))
    arrived = lax.all_to_all(
        copies.reshape(head_devices, group_rows, columns),
        "tp",
        split_axis=0,
        concat_axis=0,
        tiled=True,
    )
    parts = pl.pallas_call(
        experts,
        out_shape=jax.ShapeDtypeStruct((head_devices, group_rows, columns), jnp.bfloat16),
        in_specs=[VMEM] * 7,
        out_specs=VMEM,
        name="experts",
    )(arrived, norm_gain[None, :], packed, low, high, far_low, far_high)
    results = (
        summed_on_arrival(parts, "tp")
        .reshape(LINE, lines, group_rows, columns)
        .sum(axis=1)
        .astype(jnp.bfloat16)
        .reshape(seq_devices, slot_count, columns)
    )
    returned = lax.all_to_all(results, "sp", split_axis=0, concat_axis=0, tiled=True)
    returned_flat = returned.reshape(seq_devices * slot_count, columns).astype(jnp.float32)
    experts_sum = jnp.dot(combine, returned_flat, precision=lax.Precision.HIGHEST)
    return (stream_cols.astype(jnp.float32) + experts_sum).astype(jnp.bfloat16)


def solution(mesh):
    placed = (
        P("sp", None),
        P("sp", "tp", None),
        P("sp", "tp", None),
        P("sp", "tp", None),
        P("sp", "tp", None),
        P("sp", "tp", None),
        P("sp", "tp", None),
        P("tp"),
        P("tp"),
        P(),
        P(),
        P("tp", None),
        P("tp", None),
        P(),
        P("sp", None),
        P("sp", None),
        P("sp", None, "tp"),
        P("sp", None, "tp"),
        P("sp", "tp", None),
    )
    return jax.shard_map(
        local, mesh=mesh, in_specs=placed, out_specs=P("sp", "tp"), check_vma=False
    )
```

```python
import functools

import jax
import jax.numpy as jnp
from jax import lax
from jax.experimental import pallas as pl
from jax.experimental.pallas import tpu as pltpu
from jax.sharding import PartitionSpec as P


DK_A = 64
DK_B = 128
SEG = 64
TOP = 2
LINE = 4
EPS = 1e-06
LOW = -1e30


VMEM = pl.BlockSpec(memory_space=pltpu.VMEM)
SMEM = pl.BlockSpec(memory_space=pltpu.SMEM)
HBM = pl.BlockSpec(memory_space=pltpu.HBM)

MAPS = (
    (slice(0, 128), slice(0, 128), slice(128, 256), slice(0, 128), DK_A**-0.5),
    (slice(128, 256), slice(0, 128), slice(128, 256), slice(128, 256), DK_A**-0.5),
    (slice(256, 384), slice(256, 384), slice(512, 768), slice(256, 512), DK_B**-0.5),
    (slice(384, 512), slice(384, 512), slice(512, 768), slice(512, 768), DK_B**-0.5),
)
SUMS = 768
STATE = SUMS + 8


def absorb(first, blocks, flag_ref, own_q_ref, got_q_ref, *refs):
    kv_refs = refs[:blocks]
    olds = None if first else refs[blocks : blocks + 2]
    outs = refs[-2:]
    half = outs[0].shape[1]

    def both(refs, rows):
        return jnp.concatenate([r[rows, :] for r in refs], axis=1)

    def keep(rows, value):
        outs[0][rows, :] = value[:, :half]
        outs[1][rows, :] = value[:, half:]

    def work():
        for index, (q_cols, k_cols, v_cols, rows, factor) in enumerate(MAPS):
            keys = jnp.concatenate([r[:, k_cols] for r in kv_refs], axis=0)
            queries = jnp.concatenate([own_q_ref[:, q_cols], got_q_ref[:, q_cols]], axis=0)
            values = jnp.concatenate([r[:, v_cols] for r in kv_refs], axis=0)
            scores = (
                lax.dot_general(
                    keys,
                    queries,
                    (((1,), (1,)), ((), ())),
                    preferred_element_type=jnp.float32,
                )
                * factor
            )
            at_max = slice(SUMS + index, SUMS + index + 1)
            at_sum = slice(SUMS + 4 + index, SUMS + 5 + index)
            if first:
                key_seg = lax.broadcasted_iota(jnp.int32, scores.shape, 0) // SEG
                column = lax.broadcasted_iota(jnp.int32, scores.shape, 1)
                query_seg = jnp.where(
                    column < half, column // SEG, (column - half) // SEG + flag_ref[0]
                )
                visible = key_seg <= query_seg
                scores = jnp.where(visible, scores, LOW)
                new_max = jnp.max(scores, axis=0, keepdims=True)
                expo = jnp.where(visible, jnp.exp(scores - new_max), 0.0)
            else:
                old_max = both(olds, at_max)
                new_max = jnp.maximum(old_max, jnp.max(scores, axis=0, keepdims=True))
                expo = jnp.exp(scores - new_max)
            total = jnp.sum(expo, axis=0, keepdims=True)
            summed = lax.dot_general(
                values,
                expo.astype(jnp.bfloat16),
                (((0,), (0,)), ((), ())),
                preferred_element_type=jnp.float32,
            )
            if not first:
                shrink = jnp.exp(old_max - new_max)
                total = total + both(olds, at_sum) * shrink
                summed = summed + both(olds, rows) * shrink
            keep(rows, summed)
            keep(at_max, new_max)
            keep(at_sum, total)

    if first:
        work()
    else:
        pl.when(flag_ref[0] > 0)(work)

        @pl.when(flag_ref[0] <= 0)
        def _():
            outs[0][...] = olds[0][...]
            outs[1][...] = olds[1][...]


def absorbed(flag, queries, kvs, olds):
    half = queries[0].shape[0]
    shape = jax.ShapeDtypeStruct((STATE, half), jnp.float32)
    keys = len(kvs) * kvs[0].shape[0]
    return pl.pallas_call(
        functools.partial(absorb, olds is None, len(kvs)),
        out_shape=(shape, shape),
        in_specs=[SMEM] + [VMEM] * (2 + len(kvs) + (0 if olds is None else 2)),
        out_specs=(VMEM, VMEM),
        cost_estimate=pl.CostEstimate(
            flops=2 * 2 * half * keys * (512 + SUMS), bytes_accessed=0, transcendentals=0
        ),
        compiler_params=pltpu.CompilerParams(vmem_limit_bytes=12 << 20),
        name="absorb",
    )(flag, *queries, *kvs, *(olds or ()))


def pack(qa_ref, qb_ref, ka_ref, va_ref, kb_ref, vb_ref, q_ref, kv_ref, qa_buf, sems):
    width = qa_buf.shape[1]
    places = (
        (qa_ref, qa_buf),
        (ka_ref, kv_ref.at[:, :width]),
        (va_ref, kv_ref.at[:, width : 2 * width]),
        (kb_ref, kv_ref.at[:, 2 * width : 4 * width]),
        (vb_ref, kv_ref.at[:, 4 * width :]),
        (qb_ref, q_ref.at[:, 2 * width :]),
    )
    copies = [pltpu.make_async_copy(a, b, sems.at[i]) for i, (a, b) in enumerate(places)]
    for copy in copies:
        copy.start()
    for copy in copies:
        copy.wait()
    both = qa_buf[...]
    first = lax.broadcasted_iota(jnp.int32, both.shape, 1) < DK_A
    q_ref[:, :width] = jnp.where(first, both, 0)
    q_ref[:, width : 2 * width] = jnp.where(first, 0, both)


def pack_weights(gate_ref, up_ref, down_ref, out_ref, sems):
    deep, width = gate_ref.shape
    places = [(gate_ref, out_ref.at[:deep, :width]), (up_ref, out_ref.at[:deep, width:])]
    for j in range(deep // (2 * width)):
        start = deep + j * width
        places.append(
            (
                down_ref.at[:, 2 * j * width : 2 * (j + 1) * width],
                out_ref.at[start : start + width, :],
            )
        )
    copies = [pltpu.make_async_copy(a, b, sems.at[i]) for i, (a, b) in enumerate(places)]
    for copy in copies:
        copy.start()
    for copy in copies:
        copy.wait()


def finish(mix_ref, own_ref, got_ref, gain_a_ref, gain_b_ref, from_a_ref, from_b_ref, out_ref, *bufs):
    proj_a_ref, proj_b_ref, sems = bufs
    copy_a = pltpu.make_async_copy(from_a_ref, proj_a_ref, sems.at[0])
    copy_b = pltpu.make_async_copy(from_b_ref, proj_b_ref, sems.at[1])
    copy_a.start()
    copy_b.start()

    def merged(index):
        at_max = slice(SUMS + index, SUMS + index + 1)
        at_sum = slice(SUMS + 4 + index, SUMS + 5 + index)
        rows = MAPS[index][3]
        own_max, got_max = own_ref[at_max, :], got_ref[at_max, :]
        new_max = jnp.maximum(own_max, got_max)
        own_w, got_w = jnp.exp(own_max - new_max), jnp.exp(got_max - new_max)
        total = own_ref[at_sum, :] * own_w + got_ref[at_sum, :] * got_w
        return own_ref[rows, :] * (own_w / total) + got_ref[rows, :] * (got_w / total)

    def head(index, mixing, gain_ref):
        mixed = merged(index) - mixing * merged(index + 1)
        mean_sq = jnp.mean(mixed * mixed, axis=0, keepdims=True)
        gain = jnp.broadcast_to(gain_ref[...], mixed.shape[::-1]).T
        return (mixed * lax.rsqrt(mean_sq + EPS) * gain).astype(jnp.bfloat16)

    heads_a = head(0, mix_ref[0], gain_a_ref)
    heads_b = head(2, mix_ref[1], gain_b_ref)
    copy_a.wait()
    copy_b.wait()
    width = out_ref.shape[2]
    across = (((0,), (0,)), ((), ()))
    step = 4
    for piece in range(0, out_ref.shape[0], step):
        cols = slice(piece * width, (piece + step) * width)
        branch = lax.dot_general(
            heads_a, proj_a_ref[:, cols], across, preferred_element_type=jnp.float32
        ) + lax.dot_general(
            heads_b, proj_b_ref[:, cols], across, preferred_element_type=jnp.float32
        )
        for i in range(step):
            out_ref[piece + i] = branch[:, i * width : (i + 1) * width].astype(jnp.bfloat16)


def experts(rows_ref, gain_ref, *refs):
    froms, out_ref, bufs, sems = refs[:LINE], refs[LINE], refs[LINE + 1 : -1], refs[-1]
    copies = [pltpu.make_async_copy(a, b, sems.at[i]) for i, (a, b) in enumerate(zip(froms, bufs))]
    for copy in copies:
        copy.start()
    parts, _, width = rows_ref.shape
    model_width = parts * width
    rows = jnp.concatenate([rows_ref[i] for i in range(parts)], axis=1).astype(jnp.float32)
    mean_sq = jnp.sum(rows * rows, axis=1, keepdims=True) / model_width
    normed = (rows * lax.rsqrt(mean_sq + EPS) * gain_ref[...]).astype(jnp.bfloat16)

    def dot(a, b):
        return jnp.dot(a, b, preferred_element_type=jnp.float32)

    hidden = []
    for copy, ref in zip(copies, bufs):
        copy.wait()
        both = dot(normed, ref[:model_width, :])
        gate, up = both[:, :width], both[:, width:]
        hidden.append((gate / (1.0 + jnp.exp(-gate)) * up).astype(jnp.bfloat16))
    for j in range(parts // 2):
        start = model_width + j * width
        down = dot(hidden[0], bufs[0][start : start + width, :])
        for i in range(1, LINE):
            down = down + dot(hidden[i], bufs[i][start : start + width, :])
        out_ref[2 * j] = down[:, :width].astype(jnp.bfloat16)
        out_ref[2 * j + 1] = down[:, width:].astype(jnp.bfloat16)


def held(value):
    return pltpu.with_memory_space_constraint(value, pltpu.HBM)


def summed_on_arrival(pieces, axis):
    arrived = lax.all_to_all(pieces, axis, split_axis=0, concat_axis=0, tiled=True)
    return arrived.astype(jnp.float32)


def local(
    residual,
    query_a,
    keys_a,
    values_a,
    query_b,
    keys_b,
    values_b,
    lambda_a,
    lambda_b,
    gain_a,
    gain_b,
    proj_a,
    proj_b,
    norm_gain,
    routes,
    route_weight,
    expert_gate,
    expert_up,
    expert_down,
):
    tok_rows = residual.shape[0]
    model_width = residual.shape[1]
    seq_devices = lax.axis_size("sp")
    head_devices = lax.axis_size("tp")
    head_index = lax.axis_index("tp")
    seq_index = lax.axis_index("sp")
    columns = model_width // head_devices

    chips = seq_devices // 2
    chip, core = seq_index // 2, seq_index % 2
    partner = [(i, i ^ 1) for i in range(seq_devices)]
    half_way = chips // 2

    def onward(step, down_blocks):
        up = [(2 * i, 2 * (i + 1)) for i in range(step - 1, chips - 1)]
        places = [(block - step) % chips for block in range(down_blocks)]
        return up + [(2 * ((i + 1) % chips) + 1, 2 * i + 1) for i in places]

    fields = [a[:, 0] for a in (query_a, query_b, keys_a, values_a, keys_b, values_b)]
    own_q, own_kv = pl.pallas_call(
        pack,
        out_shape=(
            jax.ShapeDtypeStruct((tok_rows, 4 * DK_B), jnp.bfloat16),
            jax.ShapeDtypeStruct((tok_rows, SUMS), jnp.bfloat16),
        ),
        in_specs=[HBM] * 6,
        out_specs=(VMEM, VMEM),
        scratch_shapes=[pltpu.VMEM(fields[0].shape, jnp.bfloat16), pltpu.SemaphoreType.DMA((6,))],
        compiler_params=pltpu.CompilerParams(vmem_limit_bytes=8 << 20),
        name="pack",
    )(*[held(a) for a in fields])
    got_kv = lax.ppermute(own_kv, "sp", partner)
    got_q = lax.ppermute(own_q, "sp", partner)
    queries = (own_q, got_q)

    lines = head_devices // LINE
    width = expert_gate.shape[2]
    deep = expert_gate.shape[1]
    packed = pl.pallas_call(
        pack_weights,
        out_shape=pltpu.HBM((deep + deep // 2, 2 * width), jnp.bfloat16),
        in_specs=[HBM] * 3,
        out_specs=VMEM,
        scratch_shapes=[pltpu.SemaphoreType.DMA((2 + deep // (2 * width),))],
        compiler_params=pltpu.CompilerParams(vmem_limit_bytes=8 << 20),
        name="w_pack",
    )(*[held(a[0]) for a in (expert_gate, expert_up, expert_down)])
    packed = [packed]
    along = [
        (s * head_devices + t, s * head_devices + (t + (lines if s % 2 == 0 else -lines)) % head_devices)
        for s in range(seq_devices)
        for t in range(head_devices)
    ]
    for _ in range(1, LINE):
        packed.append(lax.ppermute(packed[-1], ("sp", "tp"), along))

    segments = tok_rows // SEG
    later = jnp.where(core == 0, segments, -segments).astype(jnp.int32).reshape(1)
    state = absorbed(later, queries, (own_kv,), None)
    mine, theirs = own_kv, got_kv
    for step in range(1, chips // 2 + 1):
        source = jnp.where(core == 0, chip - step, chip + step) % chips
        seen = (source < chip).astype(jnp.int32).reshape(1)
        mine = lax.ppermute(mine, "sp", onward(step, half_way))
        blocks = (mine,)
        if step < chips // 2:
            theirs = lax.ppermute(theirs, "sp", onward(step, half_way - 1))
            blocks = (mine, theirs)
        state = absorbed(seen, queries, blocks, state)
    got_state = lax.ppermute(state[1], "sp", partner)
    pieces = pl.pallas_call(
        finish,
        out_shape=jax.ShapeDtypeStruct((head_devices, tok_rows, columns), jnp.bfloat16),
        in_specs=[SMEM] + [VMEM] * 4 + [HBM] * 2,
        out_specs=VMEM,
        scratch_shapes=[
            pltpu.VMEM(proj_a.shape, jnp.bfloat16),
            pltpu.VMEM(proj_b.shape, jnp.bfloat16),
            pltpu.SemaphoreType.DMA((2,)),
        ],
        cost_estimate=pl.CostEstimate(
            flops=2 * tok_rows * model_width * 384, bytes_accessed=0, transcendentals=0
        ),
        compiler_params=pltpu.CompilerParams(vmem_limit_bytes=16 << 20),
        name="finish",
    )(
        jnp.concatenate([lambda_a, lambda_b]),
        state[0],
        got_state,
        gain_a[None, :],
        gain_b[None, :],
        held(proj_a),
        held(proj_b),
    )

    col_start = head_index * columns
    summed_cols = summed_on_arrival(pieces, "tp").sum(axis=0)
    residual_cols = lax.dynamic_slice_in_dim(residual, col_start, columns, 1)
    stream_cols = (residual_cols.astype(jnp.float32) + summed_cols).astype(jnp.bfloat16)
    slot_count = 2 * tok_rows * TOP // seq_devices
    assign = routes.reshape(-1)
    onehot = (assign[:, None] == jnp.arange(seq_devices, dtype=jnp.int32)[None, :]).astype(
        jnp.int32
    )
    earlier = jnp.cumsum(onehot, axis=0) - onehot
    slot_index = jnp.sum(earlier * onehot, axis=1)
    target = assign * slot_count + slot_index
    placed = (
        target[:, None] == jnp.arange(seq_devices * slot_count, dtype=jnp.int32)[None, :]
    ).reshape(tok_rows, TOP, -1)
    select = jnp.sum(placed.astype(jnp.bfloat16), axis=1)
    gates = route_weight / jnp.sum(route_weight, axis=1, keepdims=True)
    combine = jnp.sum(placed.astype(jnp.float32) * gates[:, :, None], axis=1)
    send_rows = jnp.einsum(
        "ts,td->sd", select, stream_cols, preferred_element_type=jnp.float32
    ).astype(jnp.bfloat16)
    send_rows = send_rows.reshape(seq_devices, slot_count, columns)
    routed = lax.all_to_all(send_rows, "sp", split_axis=0, concat_axis=0, tiled=True)
    group_rows = seq_devices * slot_count // LINE
    grouped = routed.reshape(LINE, 1, group_rows, columns)
    copies = jnp.broadcast_to(grouped, (LINE, lines, group_rows, columns))
    arrived = lax.all_to_all(
        copies.reshape(head_devices, group_rows, columns),
        "tp",
        split_axis=0,
        concat_axis=0,
        tiled=True,
    )
    parts = pl.pallas_call(
        experts,
        out_shape=jax.ShapeDtypeStruct((head_devices, group_rows, columns), jnp.bfloat16),
        in_specs=[VMEM] * 2 + [HBM] * LINE,
        out_specs=VMEM,
        scratch_shapes=[
            pltpu.VMEM(packed[0].shape, jnp.bfloat16) for _ in range(LINE)
        ]
        + [pltpu.SemaphoreType.DMA((LINE,))],
        cost_estimate=pl.CostEstimate(
            flops=6 * group_rows * model_width * LINE * width, bytes_accessed=0, transcendentals=0
        ),
        compiler_params=pltpu.CompilerParams(vmem_limit_bytes=24 << 20),
        name="experts",
    )(arrived, norm_gain[None, :], *[held(a) for a in packed])
    results = (
        summed_on_arrival(parts, "tp")
        .reshape(LINE, lines, group_rows, columns)
        .sum(axis=1)
        .astype(jnp.bfloat16)
        .reshape(seq_devices, slot_count, columns)
    )
    returned = lax.all_to_all(results, "sp", split_axis=0, concat_axis=0, tiled=True)
    returned_flat = returned.reshape(seq_devices * slot_count, columns).astype(jnp.float32)
    experts_sum = jnp.dot(combine, returned_flat, precision=lax.Precision.HIGHEST)
    return (stream_cols.astype(jnp.float32) + experts_sum).astype(jnp.bfloat16)


def solution(mesh):
    placed = (
        P("sp", None),
        P("sp", "tp", None),
        P("sp", "tp", None),
        P("sp", "tp", None),
        P("sp", "tp", None),
        P("sp", "tp", None),
        P("sp", "tp", None),
        P("tp"),
        P("tp"),
        P(),
        P(),
        P("tp", None),
        P("tp", None),
        P(),
        P("sp", None),
        P("sp", None),
        P("sp", None, "tp"),
        P("sp", None, "tp"),
        P("sp", "tp", None),
    )
    return jax.shard_map(
        local, mesh=mesh, in_specs=placed, out_specs=P("sp", "tp"), check_vma=False
    )
```

```python
import functools

import jax
import jax.numpy as jnp
from jax import lax
from jax.experimental import pallas as pl
from jax.experimental.pallas import tpu as pltpu
from jax.sharding import PartitionSpec as P


DK_A = 64
DK_B = 128
SEG = 64
TOP = 2
LINE = 4
EPS = 1e-06
LOW = -1e30


VMEM = pl.BlockSpec(memory_space=pltpu.VMEM)
SMEM = pl.BlockSpec(memory_space=pltpu.SMEM)
HBM = pl.BlockSpec(memory_space=pltpu.HBM)

MAPS = (
    (slice(0, 128), slice(0, 128), slice(128, 256), slice(0, 128), DK_A**-0.5),
    (slice(128, 256), slice(0, 128), slice(128, 256), slice(128, 256), DK_A**-0.5),
    (slice(256, 384), slice(256, 384), slice(512, 768), slice(256, 512), DK_B**-0.5),
    (slice(384, 512), slice(384, 512), slice(512, 768), slice(512, 768), DK_B**-0.5),
)
SUMS = 768
STATE = SUMS + 8


def absorb(first, blocks, flag_ref, own_q_ref, got_q_ref, *refs):
    kv_refs = refs[:blocks]
    olds = None if first else refs[blocks : blocks + 2]
    outs = refs[-2:]
    half = outs[0].shape[1]

    def both(refs, rows):
        return jnp.concatenate([r[rows, :] for r in refs], axis=1)

    def keep(rows, value):
        outs[0][rows, :] = value[:, :half]
        outs[1][rows, :] = value[:, half:]

    def work():
        for index, (q_cols, k_cols, v_cols, rows, factor) in enumerate(MAPS):
            keys = jnp.concatenate([r[:, k_cols] for r in kv_refs], axis=0)
            queries = jnp.concatenate([own_q_ref[:, q_cols], got_q_ref[:, q_cols]], axis=0)
            values = jnp.concatenate([r[:, v_cols] for r in kv_refs], axis=0)
            scores = (
                lax.dot_general(
                    keys,
                    queries,
                    (((1,), (1,)), ((), ())),
                    preferred_element_type=jnp.float32,
                )
                * factor
            )
            at_max = slice(SUMS + index, SUMS + index + 1)
            at_sum = slice(SUMS + 4 + index, SUMS + 5 + index)
            if first:
                key_seg = lax.broadcasted_iota(jnp.int32, scores.shape, 0) // SEG
                column = lax.broadcasted_iota(jnp.int32, scores.shape, 1)
                query_seg = jnp.where(
                    column < half, column // SEG, (column - half) // SEG + flag_ref[0]
                )
                visible = key_seg <= query_seg
                scores = jnp.where(visible, scores, LOW)
                new_max = jnp.max(scores, axis=0, keepdims=True)
                expo = jnp.where(visible, jnp.exp(scores - new_max), 0.0)
            else:
                old_max = both(olds, at_max)
                new_max = jnp.maximum(old_max, jnp.max(scores, axis=0, keepdims=True))
                expo = jnp.exp(scores - new_max)
            total = jnp.sum(expo, axis=0, keepdims=True)
            summed = lax.dot_general(
                values,
                expo.astype(jnp.bfloat16),
                (((0,), (0,)), ((), ())),
                preferred_element_type=jnp.float32,
            )
            if not first:
                shrink = jnp.exp(old_max - new_max)
                total = total + both(olds, at_sum) * shrink
                summed = summed + both(olds, rows) * shrink
            keep(rows, summed)
            keep(at_max, new_max)
            keep(at_sum, total)

    if first:
        work()
    else:
        pl.when(flag_ref[0] > 0)(work)

        @pl.when(flag_ref[0] <= 0)
        def _():
            outs[0][...] = olds[0][...]
            outs[1][...] = olds[1][...]


def absorbed(flag, queries, kvs, olds):
    half = queries[0].shape[0]
    shape = jax.ShapeDtypeStruct((STATE, half), jnp.float32)
    keys = len(kvs) * kvs[0].shape[0]
    return pl.pallas_call(
        functools.partial(absorb, olds is None, len(kvs)),
        out_shape=(shape, shape),
        in_specs=[SMEM] + [VMEM] * (2 + len(kvs) + (0 if olds is None else 2)),
        out_specs=(VMEM, VMEM),
        cost_estimate=pl.CostEstimate(
            flops=2 * 2 * half * keys * (512 + SUMS), bytes_accessed=0, transcendentals=0
        ),
        compiler_params=pltpu.CompilerParams(vmem_limit_bytes=12 << 20),
        name="absorb",
    )(flag, *queries, *kvs, *(olds or ()))


def pack(qa_ref, qb_ref, ka_ref, va_ref, kb_ref, vb_ref, q_ref, kv_ref, qa_buf, sems):
    width = qa_buf.shape[1]
    q_cols = q_ref.shape[1] - kv_ref.shape[1]
    places = (
        (qa_ref, qa_buf),
        (ka_ref, kv_ref.at[:, :width]),
        (va_ref, kv_ref.at[:, width : 2 * width]),
        (kb_ref, kv_ref.at[:, 2 * width : 4 * width]),
        (vb_ref, kv_ref.at[:, 4 * width :]),
        (qb_ref, q_ref.at[:, 2 * width : q_cols]),
    )
    copies = [pltpu.make_async_copy(a, b, sems.at[i]) for i, (a, b) in enumerate(places)]
    for copy in copies:
        copy.start()
    for copy in copies:
        copy.wait()
    both = qa_buf[...]
    first = lax.broadcasted_iota(jnp.int32, both.shape, 1) < DK_A
    q_ref[:, :width] = jnp.where(first, both, 0)
    q_ref[:, width : 2 * width] = jnp.where(first, 0, both)
    q_ref[:, q_cols:] = kv_ref[...]


def pack_weights(gate_ref, up_ref, down_ref, out_ref, buf, sems):
    deep, width = gate_ref.shape
    chunk = deep // 2
    pieces = []
    for start in range(0, deep, chunk):
        rows = slice(start, start + chunk)
        ins = [(ref.at[rows, :], buf.at[rows, cols]) for ref, cols in (
            (gate_ref, slice(0, width)),
            (up_ref, slice(width, 2 * width)),
        )]
        pieces.append((rows, ins))
    ins = []
    for j in range(deep // (2 * width)):
        start = deep + j * width
        ins.append(
            (
                down_ref.at[:, 2 * j * width : 2 * (j + 1) * width],
                buf.at[start : start + width, :],
            )
        )
    pieces.append((slice(deep, deep + deep // 2), ins))
    count, started = 0, []
    for rows, ins in pieces:
        copies = []
        for a, b in ins:
            copies.append(pltpu.make_async_copy(a, b, sems.at[count]))
            copies[-1].start()
            count += 1
        started.append((rows, copies))
    outs = []
    for rows, copies in started:
        for copy in copies:
            copy.wait()
        outs.append(pltpu.make_async_copy(buf.at[rows, :], out_ref.at[rows, :], sems.at[count]))
        outs[-1].start()
        count += 1
    for copy in outs:
        copy.wait()


def finish(mix_ref, own_ref, got_ref, gain_a_ref, gain_b_ref, from_a_ref, from_b_ref, out_ref, *bufs):
    proj_a_ref, proj_b_ref, sems = bufs
    copy_a = pltpu.make_async_copy(from_a_ref, proj_a_ref, sems.at[0])
    copy_b = pltpu.make_async_copy(from_b_ref, proj_b_ref, sems.at[1])
    copy_a.start()
    copy_b.start()

    def merged(index):
        at_max = slice(SUMS + index, SUMS + index + 1)
        at_sum = slice(SUMS + 4 + index, SUMS + 5 + index)
        rows = MAPS[index][3]
        own_max, got_max = own_ref[at_max, :], got_ref[at_max, :]
        new_max = jnp.maximum(own_max, got_max)
        own_w, got_w = jnp.exp(own_max - new_max), jnp.exp(got_max - new_max)
        total = own_ref[at_sum, :] * own_w + got_ref[at_sum, :] * got_w
        return own_ref[rows, :] * (own_w / total) + got_ref[rows, :] * (got_w / total)

    def head(index, mixing, gain_ref):
        mixed = merged(index) - mixing * merged(index + 1)
        mean_sq = jnp.mean(mixed * mixed, axis=0, keepdims=True)
        gain = jnp.broadcast_to(gain_ref[...], mixed.shape[::-1]).T
        return (mixed * lax.rsqrt(mean_sq + EPS) * gain).astype(jnp.bfloat16)

    heads_a = head(0, mix_ref[0], gain_a_ref)
    heads_b = head(2, mix_ref[1], gain_b_ref)
    copy_a.wait()
    copy_b.wait()
    width = out_ref.shape[2]
    across = (((0,), (0,)), ((), ()))
    step = 4
    for piece in range(0, out_ref.shape[0], step):
        cols = slice(piece * width, (piece + step) * width)
        branch = lax.dot_general(
            heads_a, proj_a_ref[:, cols], across, preferred_element_type=jnp.float32
        ) + lax.dot_general(
            heads_b, proj_b_ref[:, cols], across, preferred_element_type=jnp.float32
        )
        for i in range(step):
            out_ref[piece + i] = branch[:, i * width : (i + 1) * width].astype(jnp.bfloat16)


def experts(rows_ref, gain_ref, *refs):
    here, froms, out_ref, bufs, sems = refs[0], refs[1:LINE], refs[LINE], refs[LINE + 1 : -1], refs[-1]
    copies = [pltpu.make_async_copy(a, b, sems.at[i]) for i, (a, b) in enumerate(zip(froms, bufs))]
    for copy in copies:
        copy.start()
    parts, _, width = rows_ref.shape
    model_width = parts * width
    rows = jnp.concatenate([rows_ref[i] for i in range(parts)], axis=1).astype(jnp.float32)
    mean_sq = jnp.sum(rows * rows, axis=1, keepdims=True) / model_width
    normed = (rows * lax.rsqrt(mean_sq + EPS) * gain_ref[...]).astype(jnp.bfloat16)

    def dot(a, b):
        return jnp.dot(a, b, preferred_element_type=jnp.float32)

    hidden = []
    bufs = (here, *bufs)
    for index, ref in enumerate(bufs):
        if index > 0:
            copies[index - 1].wait()
        both = dot(normed, ref[:model_width, :])
        gate, up = both[:, :width], both[:, width:]
        hidden.append((gate / (1.0 + jnp.exp(-gate)) * up).astype(jnp.bfloat16))
    for j in range(parts // 2):
        start = model_width + j * width
        down = dot(hidden[0], bufs[0][start : start + width, :])
        for i in range(1, LINE):
            down = down + dot(hidden[i], bufs[i][start : start + width, :])
        out_ref[2 * j] = down[:, :width].astype(jnp.bfloat16)
        out_ref[2 * j + 1] = down[:, width:].astype(jnp.bfloat16)


def held(value):
    return pltpu.with_memory_space_constraint(value, pltpu.HBM)


def summed_on_arrival(pieces, axis):
    arrived = lax.all_to_all(pieces, axis, split_axis=0, concat_axis=0, tiled=True)
    return arrived.astype(jnp.float32)


def local(
    residual,
    query_a,
    keys_a,
    values_a,
    query_b,
    keys_b,
    values_b,
    lambda_a,
    lambda_b,
    gain_a,
    gain_b,
    proj_a,
    proj_b,
    norm_gain,
    routes,
    route_weight,
    expert_gate,
    expert_up,
    expert_down,
):
    tok_rows = residual.shape[0]
    model_width = residual.shape[1]
    seq_devices = lax.axis_size("sp")
    head_devices = lax.axis_size("tp")
    head_index = lax.axis_index("tp")
    seq_index = lax.axis_index("sp")
    columns = model_width // head_devices

    chips = seq_devices // 2
    chip, core = seq_index // 2, seq_index % 2
    partner = [(i, i ^ 1) for i in range(seq_devices)]
    half_way = chips // 2

    def onward(step):
        up = [(2 * i + 1, 2 * (i + 1) + 1) for i in range(step - 1, chips - 1)]
        places = [(block - step) % chips for block in range(half_way - 1)] if step < half_way else []
        return up + [(2 * ((i + 1) % chips), 2 * i) for i in places]

    fields = [a[:, 0] for a in (query_a, query_b, keys_a, values_a, keys_b, values_b)]
    own_all, own_kv = pl.pallas_call(
        pack,
        out_shape=(
            jax.ShapeDtypeStruct((tok_rows, 4 * DK_B + SUMS), jnp.bfloat16),
            jax.ShapeDtypeStruct((tok_rows, SUMS), jnp.bfloat16),
        ),
        in_specs=[HBM] * 6,
        out_specs=(VMEM, VMEM),
        scratch_shapes=[pltpu.VMEM(fields[0].shape, jnp.bfloat16), pltpu.SemaphoreType.DMA((6,))],
        compiler_params=pltpu.CompilerParams(vmem_limit_bytes=8 << 20),
        name="pack",
    )(*[held(a) for a in fields])
    got_all = lax.ppermute(own_all, "sp", partner)
    got_kv = got_all[:, 4 * DK_B :]
    queries = (own_all, got_all)

    lines = head_devices // LINE
    width = expert_gate.shape[2]
    deep = expert_gate.shape[1]
    packed = pl.pallas_call(
        pack_weights,
        out_shape=pltpu.HBM((deep + deep // 2, 2 * width), jnp.bfloat16),
        in_specs=[HBM] * 3,
        out_specs=HBM,
        scratch_shapes=[
            pltpu.VMEM((deep + deep // 2, 2 * width), jnp.bfloat16),
            pltpu.SemaphoreType.DMA((4 + deep // (2 * width) + 3,)),
        ],
        compiler_params=pltpu.CompilerParams(vmem_limit_bytes=8 << 20),
        name="w_pack",
    )(*[held(a[0]) for a in (expert_gate, expert_up, expert_down)])
    packed = [packed]
    along = [
        (s * head_devices + t, s * head_devices + (t + (lines if s % 2 == 0 else -lines)) % head_devices)
        for s in range(seq_devices)
        for t in range(head_devices)
    ]
    for _ in range(1, LINE):
        packed.append(lax.ppermute(packed[-1], ("sp", "tp"), along))

    segments = tok_rows // SEG
    later = jnp.where(core == 0, segments, -segments).astype(jnp.int32).reshape(1)
    state = absorbed(later, queries, (own_kv,), None)
    mine, theirs = own_kv, got_kv
    for step in range(1, half_way + 1):
        source = jnp.where(core == 1, chip - step, chip + step) % chips
        seen = ((source < chip) & ((core == 1) | (step < half_way))).astype(jnp.int32).reshape(1)
        mine = lax.ppermute(mine, "sp", onward(step))
        theirs = lax.ppermute(theirs, "sp", onward(step))
        state = absorbed(seen, queries, (mine, theirs), state)
    got_state = lax.ppermute(state[1], "sp", partner)
    pieces = pl.pallas_call(
        finish,
        out_shape=pltpu.VMEM((head_devices, tok_rows, columns), jnp.bfloat16),
        in_specs=[SMEM] + [VMEM] * 4 + [HBM] * 2,
        out_specs=VMEM,
        scratch_shapes=[
            pltpu.VMEM(proj_a.shape, jnp.bfloat16),
            pltpu.VMEM(proj_b.shape, jnp.bfloat16),
            pltpu.SemaphoreType.DMA((2,)),
        ],
        cost_estimate=pl.CostEstimate(
            flops=2 * tok_rows * model_width * 384, bytes_accessed=0, transcendentals=0
        ),
        compiler_params=pltpu.CompilerParams(vmem_limit_bytes=16 << 20),
        name="finish",
    )(
        jnp.concatenate([lambda_a, lambda_b]),
        state[0],
        got_state,
        gain_a[None, :],
        gain_b[None, :],
        held(proj_a),
        held(proj_b),
    )

    col_start = head_index * columns
    arrived = lax.all_to_all(pieces, "tp", split_axis=0, concat_axis=0, tiled=True)
    summed_cols = arrived.astype(jnp.float32).sum(axis=0)
    residual_cols = lax.dynamic_slice_in_dim(residual, col_start, columns, 1)
    stream_cols = (residual_cols.astype(jnp.float32) + summed_cols).astype(jnp.bfloat16)
    slot_count = 2 * tok_rows * TOP // seq_devices
    assign = routes.reshape(-1)
    onehot = (assign[:, None] == jnp.arange(seq_devices, dtype=jnp.int32)[None, :]).astype(
        jnp.int32
    )
    earlier = jnp.cumsum(onehot, axis=0) - onehot
    slot_index = jnp.sum(earlier * onehot, axis=1)
    target = assign * slot_count + slot_index
    placed = (
        target[:, None] == jnp.arange(seq_devices * slot_count, dtype=jnp.int32)[None, :]
    ).reshape(tok_rows, TOP, -1)
    select = jnp.sum(placed.astype(jnp.bfloat16), axis=1)
    gates = route_weight / jnp.sum(route_weight, axis=1, keepdims=True)
    combine = jnp.sum(placed.astype(jnp.float32) * gates[:, :, None], axis=1)
    send_rows = jnp.einsum(
        "ts,td->sd", select, stream_cols, preferred_element_type=jnp.float32
    ).astype(jnp.bfloat16)
    send_rows = send_rows.reshape(seq_devices, slot_count, columns)
    routed = lax.all_to_all(send_rows, "sp", split_axis=0, concat_axis=0, tiled=True)
    group_rows = seq_devices * slot_count // LINE
    grouped = routed.reshape(LINE, 1, group_rows, columns)
    copies = jnp.broadcast_to(grouped, (LINE, lines, group_rows, columns))
    arrived = lax.all_to_all(
        copies.reshape(head_devices, group_rows, columns),
        "tp",
        split_axis=0,
        concat_axis=0,
        tiled=True,
    )
    parts = pl.pallas_call(
        experts,
        out_shape=jax.ShapeDtypeStruct((head_devices, group_rows, columns), jnp.bfloat16),
        in_specs=[VMEM] * 3 + [HBM] * (LINE - 1),
        out_specs=VMEM,
        scratch_shapes=[
            pltpu.VMEM(packed[0].shape, jnp.bfloat16) for _ in range(LINE - 1)
        ]
        + [pltpu.SemaphoreType.DMA((LINE - 1,))],
        cost_estimate=pl.CostEstimate(
            flops=6 * group_rows * model_width * LINE * width, bytes_accessed=0, transcendentals=0
        ),
        compiler_params=pltpu.CompilerParams(vmem_limit_bytes=24 << 20),
        name="experts",
    )(arrived, norm_gain[None, :], packed[-1], *[held(a) for a in packed[:-1]])
    results = (
        summed_on_arrival(parts, "tp")
        .reshape(LINE, lines, group_rows, columns)
        .sum(axis=1)
        .astype(jnp.bfloat16)
        .reshape(seq_devices, slot_count, columns)
    )
    returned = lax.all_to_all(results, "sp", split_axis=0, concat_axis=0, tiled=True)
    returned_flat = returned.reshape(seq_devices * slot_count, columns).astype(jnp.float32)
    experts_sum = jnp.dot(combine, returned_flat, precision=lax.Precision.HIGHEST)
    return (stream_cols.astype(jnp.float32) + experts_sum).astype(jnp.bfloat16)


def solution(mesh):
    placed = (
        P("sp", None),
        P("sp", "tp", None),
        P("sp", "tp", None),
        P("sp", "tp", None),
        P("sp", "tp", None),
        P("sp", "tp", None),
        P("sp", "tp", None),
        P("tp"),
        P("tp"),
        P(),
        P(),
        P("tp", None),
        P("tp", None),
        P(),
        P("sp", None),
        P("sp", None),
        P("sp", None, "tp"),
        P("sp", None, "tp"),
        P("sp", "tp", None),
    )
    return jax.shard_map(
        local, mesh=mesh, in_specs=placed, out_specs=P("sp", "tp"), check_vma=False
    )
```

```python
import functools

import jax
import jax.numpy as jnp
from jax import lax
from jax.experimental import pallas as pl
from jax.experimental.pallas import tpu as pltpu
from jax.sharding import PartitionSpec as P


DK_A = 64
DK_B = 128
SEG = 64
TOP = 2
LINE = 4
EPS = 1e-06
LOW = -1e30


VMEM = pl.BlockSpec(memory_space=pltpu.VMEM)
SMEM = pl.BlockSpec(memory_space=pltpu.SMEM)
HBM = pl.BlockSpec(memory_space=pltpu.HBM)

MAPS = (
    (slice(0, 128), slice(0, 128), slice(128, 256), slice(0, 128), DK_A**-0.5),
    (slice(128, 256), slice(0, 128), slice(128, 256), slice(128, 256), DK_A**-0.5),
    (slice(256, 384), slice(256, 384), slice(512, 768), slice(256, 512), DK_B**-0.5),
    (slice(384, 512), slice(384, 512), slice(512, 768), slice(512, 768), DK_B**-0.5),
)
SUMS = 768
STATE = SUMS + 8


def absorb(first, blocks, flag_ref, own_q_ref, got_q_ref, *refs):
    kv_refs = refs[:blocks]
    olds = None if first else refs[blocks : blocks + 2]
    outs = refs[-2:]
    half = outs[0].shape[1]

    def both(refs, rows):
        return jnp.concatenate([r[rows, :] for r in refs], axis=1)

    def keep(rows, value):
        outs[0][rows, :] = value[:, :half]
        outs[1][rows, :] = value[:, half:]

    def work():
        for index, (q_cols, k_cols, v_cols, rows, factor) in enumerate(MAPS):
            keys = jnp.concatenate([r[:, k_cols] for r in kv_refs], axis=0)
            queries = jnp.concatenate([own_q_ref[:, q_cols], got_q_ref[:, q_cols]], axis=0)
            values = jnp.concatenate([r[:, v_cols] for r in kv_refs], axis=0)
            scores = (
                lax.dot_general(
                    keys,
                    queries,
                    (((1,), (1,)), ((), ())),
                    preferred_element_type=jnp.float32,
                )
                * factor
            )
            at_max = slice(SUMS + index, SUMS + index + 1)
            at_sum = slice(SUMS + 4 + index, SUMS + 5 + index)
            if first:
                key_seg = lax.broadcasted_iota(jnp.int32, scores.shape, 0) // SEG
                column = lax.broadcasted_iota(jnp.int32, scores.shape, 1)
                query_seg = jnp.where(
                    column < half, column // SEG, (column - half) // SEG + flag_ref[0]
                )
                visible = key_seg <= query_seg
                scores = jnp.where(visible, scores, LOW)
                new_max = jnp.max(scores, axis=0, keepdims=True)
                expo = jnp.where(visible, jnp.exp(scores - new_max), 0.0)
            else:
                old_max = both(olds, at_max)
                new_max = jnp.maximum(old_max, jnp.max(scores, axis=0, keepdims=True))
                expo = jnp.exp(scores - new_max)
            total = jnp.sum(expo, axis=0, keepdims=True)
            summed = lax.dot_general(
                values,
                expo.astype(jnp.bfloat16),
                (((0,), (0,)), ((), ())),
                preferred_element_type=jnp.float32,
            )
            if not first:
                shrink = jnp.exp(old_max - new_max)
                total = total + both(olds, at_sum) * shrink
                summed = summed + both(olds, rows) * shrink
            keep(rows, summed)
            keep(at_max, new_max)
            keep(at_sum, total)

    if first:
        work()
    else:
        pl.when(flag_ref[0] > 0)(work)

        @pl.when(flag_ref[0] <= 0)
        def _():
            outs[0][...] = olds[0][...]
            outs[1][...] = olds[1][...]


def absorbed(flag, queries, kvs, olds):
    half = queries[0].shape[0]
    shape = jax.ShapeDtypeStruct((STATE, half), jnp.float32)
    keys = len(kvs) * kvs[0].shape[0]
    return pl.pallas_call(
        functools.partial(absorb, olds is None, len(kvs)),
        out_shape=(shape, shape),
        in_specs=[SMEM] + [VMEM] * (2 + len(kvs) + (0 if olds is None else 2)),
        out_specs=(VMEM, VMEM),
        cost_estimate=pl.CostEstimate(
            flops=2 * 2 * half * keys * (512 + SUMS), bytes_accessed=0, transcendentals=0
        ),
        compiler_params=pltpu.CompilerParams(vmem_limit_bytes=12 << 20),
        name="absorb",
    )(flag, *queries, *kvs, *(olds or ()))


def pack(qa_ref, qb_ref, ka_ref, va_ref, kb_ref, vb_ref, gate_ref, up_ref, down_ref, *refs):
    q_ref, kv_ref, out_ref, qa_buf, buf, sems = refs
    width = qa_buf.shape[1]
    q_cols = q_ref.shape[1] - kv_ref.shape[1]
    deep, wide = gate_ref.shape
    count = 0

    def begin(places):
        nonlocal count
        copies = []
        for a, b in places:
            copies.append(pltpu.make_async_copy(a, b, sems.at[count]))
            copies[-1].start()
            count += 1
        return copies

    first = begin(
        (
            (qa_ref, qa_buf),
            (ka_ref, kv_ref.at[:, :width]),
            (va_ref, kv_ref.at[:, width : 2 * width]),
            (kb_ref, kv_ref.at[:, 2 * width : 4 * width]),
            (vb_ref, kv_ref.at[:, 4 * width :]),
            (qb_ref, q_ref.at[:, 2 * width : q_cols]),
        )
    )
    pieces = []
    chunk = deep // 2
    for start in range(0, deep, chunk):
        rows = slice(start, start + chunk)
        sides = ((gate_ref, slice(0, wide)), (up_ref, slice(wide, 2 * wide)))
        pieces.append((rows, begin([(ref.at[rows, :], buf.at[rows, cols]) for ref, cols in sides])))
    places = []
    for j in range(deep // (2 * wide)):
        start = deep + j * wide
        cols = slice(2 * j * wide, 2 * (j + 1) * wide)
        places.append((down_ref.at[:, cols], buf.at[start : start + wide, :]))
    pieces.append((slice(deep, deep + deep // 2), begin(places)))
    for copy in first:
        copy.wait()
    both = qa_buf[...]
    first_map = lax.broadcasted_iota(jnp.int32, both.shape, 1) < DK_A
    q_ref[:, :width] = jnp.where(first_map, both, 0)
    q_ref[:, width : 2 * width] = jnp.where(first_map, 0, both)
    q_ref[:, q_cols:] = kv_ref[...]
    outs = []
    for rows, copies in pieces:
        for copy in copies:
            copy.wait()
        outs += begin([(buf.at[rows, :], out_ref.at[rows, :])])
    for copy in outs:
        copy.wait()


def fetch(*refs):
    count = (len(refs) - 1) // 2
    sems = refs[-1]
    copies = [pltpu.make_async_copy(refs[i], refs[count + i], sems.at[i]) for i in range(count)]
    for copy in copies:
        copy.start()
    for copy in copies:
        copy.wait()


def finish(mix_ref, at_ref, own_ref, got_ref, *refs):
    gain_a_ref, gain_b_ref, proj_a_ref, proj_b_ref, residual_ref, out_ref, cols_ref, sem = refs
    start = pl.multiple_of(at_ref[0] * cols_ref.shape[1], cols_ref.shape[1])
    copy = pltpu.make_async_copy(
        residual_ref.at[:, pl.ds(start, cols_ref.shape[1])], cols_ref, sem
    )
    copy.start()

    def merged(index):
        at_max = slice(SUMS + index, SUMS + index + 1)
        at_sum = slice(SUMS + 4 + index, SUMS + 5 + index)
        rows = MAPS[index][3]
        own_max, got_max = own_ref[at_max, :], got_ref[at_max, :]
        new_max = jnp.maximum(own_max, got_max)
        own_w, got_w = jnp.exp(own_max - new_max), jnp.exp(got_max - new_max)
        total = own_ref[at_sum, :] * own_w + got_ref[at_sum, :] * got_w
        return own_ref[rows, :] * (own_w / total) + got_ref[rows, :] * (got_w / total)

    def head(index, mixing, gain_ref):
        mixed = merged(index) - mixing * merged(index + 1)
        mean_sq = jnp.mean(mixed * mixed, axis=0, keepdims=True)
        gain = jnp.broadcast_to(gain_ref[...], mixed.shape[::-1]).T
        return (mixed * lax.rsqrt(mean_sq + EPS) * gain).astype(jnp.bfloat16)

    heads_a = head(0, mix_ref[0], gain_a_ref)
    heads_b = head(2, mix_ref[1], gain_b_ref)
    width = out_ref.shape[2]
    across = (((0,), (0,)), ((), ()))
    step = 4
    for piece in range(0, out_ref.shape[0], step):
        cols = slice(piece * width, (piece + step) * width)
        branch = lax.dot_general(
            heads_a, proj_a_ref[:, cols], across, preferred_element_type=jnp.float32
        ) + lax.dot_general(
            heads_b, proj_b_ref[:, cols], across, preferred_element_type=jnp.float32
        )
        for i in range(step):
            out_ref[piece + i] = branch[:, i * width : (i + 1) * width].astype(jnp.bfloat16)
    copy.wait()


def place(arrived_ref, residual_ref, select_ref, stream_ref, send_ref):
    summed = arrived_ref[0].astype(jnp.float32)
    for i in range(1, arrived_ref.shape[0]):
        summed = summed + arrived_ref[i].astype(jnp.float32)
    stream = (residual_ref[...].astype(jnp.float32) + summed).astype(jnp.bfloat16)
    stream_ref[...] = stream
    send_ref[...] = lax.dot_general(
        select_ref[...], stream, (((0,), (0,)), ((), ())), preferred_element_type=jnp.float32
    ).astype(jnp.bfloat16)


def experts(rows_ref, gain_ref, *refs):
    here, froms, out_ref, bufs, sems = refs[0], refs[1:LINE], refs[LINE], refs[LINE + 1 : -1], refs[-1]
    copies = [pltpu.make_async_copy(a, b, sems.at[i]) for i, (a, b) in enumerate(zip(froms, bufs))]
    for copy in copies:
        copy.start()
    parts, _, width = rows_ref.shape
    model_width = parts * width
    rows = jnp.concatenate([rows_ref[i] for i in range(parts)], axis=1).astype(jnp.float32)
    mean_sq = jnp.sum(rows * rows, axis=1, keepdims=True) / model_width
    normed = (rows * lax.rsqrt(mean_sq + EPS) * gain_ref[...]).astype(jnp.bfloat16)

    def dot(a, b):
        return jnp.dot(a, b, preferred_element_type=jnp.float32)

    hidden = []
    bufs = (here, *bufs)
    for index, ref in enumerate(bufs):
        if index > 0:
            copies[index - 1].wait()
        both = dot(normed, ref[:model_width, :])
        gate, up = both[:, :width], both[:, width:]
        hidden.append((gate / (1.0 + jnp.exp(-gate)) * up).astype(jnp.bfloat16))
    for j in range(parts // 2):
        start = model_width + j * width
        down = dot(hidden[0], bufs[0][start : start + width, :])
        for i in range(1, LINE):
            down = down + dot(hidden[i], bufs[i][start : start + width, :])
        out_ref[2 * j] = down[:, :width].astype(jnp.bfloat16)
        out_ref[2 * j + 1] = down[:, width:].astype(jnp.bfloat16)


def held(value):
    return pltpu.with_memory_space_constraint(value, pltpu.HBM)


def summed_on_arrival(pieces, axis):
    arrived = lax.all_to_all(pieces, axis, split_axis=0, concat_axis=0, tiled=True)
    return arrived.astype(jnp.float32)


def local(
    residual,
    query_a,
    keys_a,
    values_a,
    query_b,
    keys_b,
    values_b,
    lambda_a,
    lambda_b,
    gain_a,
    gain_b,
    proj_a,
    proj_b,
    norm_gain,
    routes,
    route_weight,
    expert_gate,
    expert_up,
    expert_down,
):
    tok_rows = residual.shape[0]
    model_width = residual.shape[1]
    seq_devices = lax.axis_size("sp")
    head_devices = lax.axis_size("tp")
    head_index = lax.axis_index("tp")
    seq_index = lax.axis_index("sp")
    columns = model_width // head_devices

    chips = seq_devices // 2
    chip, core = seq_index // 2, seq_index % 2
    partner = [(i, i ^ 1) for i in range(seq_devices)]
    half_way = chips // 2

    quarter = half_way // 2

    def onward(step, up_blocks, down_blocks):
        up = [block + step for block in up_blocks if block + step < chips]
        down = [(block - step) % chips for block in down_blocks]
        return [(2 * i - 1, 2 * i + 1) for i in up] + [(2 * ((i + 1) % chips), 2 * i) for i in down]

    fields = [a[:, 0] for a in (query_a, query_b, keys_a, values_a, keys_b, values_b)]
    deep, width = expert_gate.shape[1:]
    weights = [a[0] for a in (expert_gate, expert_up, expert_down)]
    own_all, own_kv, packed = pl.pallas_call(
        pack,
        out_shape=(
            jax.ShapeDtypeStruct((tok_rows, 4 * DK_B + SUMS), jnp.bfloat16),
            jax.ShapeDtypeStruct((tok_rows, SUMS), jnp.bfloat16),
            pltpu.HBM((deep + deep // 2, 2 * width), jnp.bfloat16),
        ),
        in_specs=[HBM] * 9,
        out_specs=(VMEM, VMEM, HBM),
        scratch_shapes=[
            pltpu.VMEM(fields[0].shape, jnp.bfloat16),
            pltpu.VMEM((deep + deep // 2, 2 * width), jnp.bfloat16),
            pltpu.SemaphoreType.DMA((6 + 4 + deep // (2 * width) + 3,)),
        ],
        compiler_params=pltpu.CompilerParams(vmem_limit_bytes=8 << 20),
        name="pack",
    )(*[held(a) for a in fields + weights])
    got_all = lax.ppermute(own_all, "sp", partner)
    got_kv = got_all[:, 4 * DK_B :]
    queries = (own_all, got_all)

    lines = head_devices // LINE
    packed = [packed]
    along = [
        (s * head_devices + t, s * head_devices + (t + (lines if s % 2 == 0 else -lines)) % head_devices)
        for s in range(seq_devices)
        for t in range(head_devices)
    ]
    for _ in range(1, LINE):
        packed.append(lax.ppermute(packed[-1], ("sp", "tp"), along))

    segments = tok_rows // SEG
    later = jnp.where(core == 0, segments, -segments).astype(jnp.int32).reshape(1)
    state = absorbed(later, queries, (own_kv,), None)
    mine, theirs = own_kv, got_kv
    for step in range(1, half_way):
        source = jnp.where(core == 1, chip - step, chip + step) % chips
        seen = (source < chip).astype(jnp.int32).reshape(1)
        pairs = onward(step, range(chips), range(half_way - 1))
        mine = lax.ppermute(mine, "sp", pairs)
        theirs = lax.ppermute(theirs, "sp", pairs)
        state = absorbed(seen, queries, (mine, theirs), state)
    near = (chip >= half_way) & (chip < half_way + quarter)
    mine = lax.ppermute(mine, "sp", onward(half_way, range(half_way), range(quarter)))
    theirs = lax.ppermute(theirs, "sp", onward(half_way, range(quarter, half_way), ()))
    seen = jnp.where(core == 1, chip >= half_way, near).astype(jnp.int32).reshape(1)
    state = absorbed(seen, queries, (mine,), state)
    seen = ((core == 1) & (chip >= half_way + quarter)).astype(jnp.int32).reshape(1)
    state = absorbed(seen, queries, (theirs,), state)
    got_state = lax.ppermute(state[1], "sp", partner)
    projs = pl.pallas_call(
        fetch,
        out_shape=tuple(pltpu.VMEM(a.shape, jnp.bfloat16) for a in (proj_a, proj_b)),
        in_specs=[HBM] * 2,
        out_specs=(VMEM, VMEM),
        scratch_shapes=[pltpu.SemaphoreType.DMA((2,))],
        compiler_params=pltpu.CompilerParams(vmem_limit_bytes=4 << 20),
        name="fetch",
    )(held(proj_a), held(proj_b))
    mix = jnp.concatenate([lambda_a, lambda_b])
    pieces, residual_cols = pl.pallas_call(
        finish,
        out_shape=(
            jax.ShapeDtypeStruct((head_devices, tok_rows, columns), jnp.bfloat16),
            jax.ShapeDtypeStruct((tok_rows, columns), jnp.bfloat16),
        ),
        in_specs=[SMEM] * 2 + [VMEM] * 6 + [HBM],
        out_specs=(VMEM, VMEM),
        scratch_shapes=[pltpu.SemaphoreType.DMA],
        cost_estimate=pl.CostEstimate(
            flops=2 * tok_rows * model_width * 384, bytes_accessed=0, transcendentals=0
        ),
        compiler_params=pltpu.CompilerParams(vmem_limit_bytes=16 << 20),
        name="finish",
    )(
        mix,
        head_index.astype(jnp.int32).reshape(1),
        state[0],
        got_state,
        gain_a[None, :],
        gain_b[None, :],
        *projs,
        held(residual),
    )

    arrived = lax.all_to_all(pieces, "tp", split_axis=0, concat_axis=0, tiled=True)
    slot_count = 2 * tok_rows * TOP // seq_devices
    assign = routes.reshape(-1)
    onehot = (assign[:, None] == jnp.arange(seq_devices, dtype=jnp.int32)[None, :]).astype(
        jnp.int32
    )
    earlier = jnp.cumsum(onehot, axis=0) - onehot
    slot_index = jnp.sum(earlier * onehot, axis=1)
    target = assign * slot_count + slot_index
    placed = (
        target[:, None] == jnp.arange(seq_devices * slot_count, dtype=jnp.int32)[None, :]
    ).reshape(tok_rows, TOP, -1)
    select = jnp.sum(placed.astype(jnp.bfloat16), axis=1)
    gates = route_weight / jnp.sum(route_weight, axis=1, keepdims=True)
    combine = jnp.sum(placed.astype(jnp.float32) * gates[:, :, None], axis=1)
    stream_cols, send_rows = pl.pallas_call(
        place,
        out_shape=(
            jax.ShapeDtypeStruct((tok_rows, columns), jnp.bfloat16),
            jax.ShapeDtypeStruct((seq_devices * slot_count, columns), jnp.bfloat16),
        ),
        in_specs=[VMEM] * 3,
        out_specs=(VMEM, VMEM),
        compiler_params=pltpu.CompilerParams(vmem_limit_bytes=4 << 20),
        name="place",
    )(arrived, residual_cols, select)
    send_rows = send_rows.reshape(seq_devices, slot_count, columns)
    routed = lax.all_to_all(send_rows, "sp", split_axis=0, concat_axis=0, tiled=True)
    group_rows = seq_devices * slot_count // LINE
    grouped = routed.reshape(LINE, 1, group_rows, columns)
    copies = jnp.broadcast_to(grouped, (LINE, lines, group_rows, columns))
    arrived = lax.all_to_all(
        copies.reshape(head_devices, group_rows, columns),
        "tp",
        split_axis=0,
        concat_axis=0,
        tiled=True,
    )
    parts = pl.pallas_call(
        experts,
        out_shape=jax.ShapeDtypeStruct((head_devices, group_rows, columns), jnp.bfloat16),
        in_specs=[VMEM] * 3 + [HBM] * (LINE - 1),
        out_specs=VMEM,
        scratch_shapes=[
            pltpu.VMEM(packed[0].shape, jnp.bfloat16) for _ in range(LINE - 1)
        ]
        + [pltpu.SemaphoreType.DMA((LINE - 1,))],
        cost_estimate=pl.CostEstimate(
            flops=6 * group_rows * model_width * LINE * width, bytes_accessed=0, transcendentals=0
        ),
        compiler_params=pltpu.CompilerParams(vmem_limit_bytes=24 << 20),
        name="experts",
    )(arrived, norm_gain[None, :], packed[-1], *[held(a) for a in packed[:-1]])
    results = (
        summed_on_arrival(parts, "tp")
        .reshape(LINE, lines, group_rows, columns)
        .sum(axis=1)
        .astype(jnp.bfloat16)
        .reshape(seq_devices, slot_count, columns)
    )
    returned = lax.all_to_all(results, "sp", split_axis=0, concat_axis=0, tiled=True)
    returned_flat = returned.reshape(seq_devices * slot_count, columns).astype(jnp.float32)
    experts_sum = jnp.dot(combine, returned_flat, precision=lax.Precision.HIGHEST)
    return (stream_cols.astype(jnp.float32) + experts_sum).astype(jnp.bfloat16)


def solution(mesh):
    placed = (
        P("sp", None),
        P("sp", "tp", None),
        P("sp", "tp", None),
        P("sp", "tp", None),
        P("sp", "tp", None),
        P("sp", "tp", None),
        P("sp", "tp", None),
        P("tp"),
        P("tp"),
        P(),
        P(),
        P("tp", None),
        P("tp", None),
        P(),
        P("sp", None),
        P("sp", None),
        P("sp", None, "tp"),
        P("sp", None, "tp"),
        P("sp", "tp", None),
    )
    return jax.shard_map(
        local, mesh=mesh, in_specs=placed, out_specs=P("sp", "tp"), check_vma=False
    )
```

```python
import functools

import jax
import jax.numpy as jnp
from jax import lax
from jax.experimental import pallas as pl
from jax.experimental.pallas import tpu as pltpu
from jax.sharding import Mesh
from jax.sharding import PartitionSpec as P


DK_A = 64
DK_B = 128
SEG = 64
TOP = 2
LINE = 4
EPS = 1e-06
LOW = -1e30


VMEM = pl.BlockSpec(memory_space=pltpu.VMEM)
SMEM = pl.BlockSpec(memory_space=pltpu.SMEM)
HBM = pl.BlockSpec(memory_space=pltpu.HBM)

MAPS = (
    (slice(0, 128), slice(0, 128), slice(128, 256), slice(0, 128), DK_A**-0.5),
    (slice(128, 256), slice(0, 128), slice(128, 256), slice(128, 256), DK_A**-0.5),
    (slice(256, 384), slice(256, 384), slice(512, 768), slice(256, 512), DK_B**-0.5),
    (slice(384, 512), slice(384, 512), slice(512, 768), slice(512, 768), DK_B**-0.5),
)
SUMS = 768
SEQ = ("z", "core")
STATE = SUMS + 8


def absorb(first, blocks, flag_ref, own_q_ref, got_q_ref, *refs):
    kv_refs = refs[:blocks]
    olds = None if first else refs[blocks : blocks + 2]
    outs = refs[-2:]
    half = outs[0].shape[1]

    def both(refs, rows):
        return jnp.concatenate([r[rows, :] for r in refs], axis=1)

    def keep(rows, value):
        outs[0][rows, :] = value[:, :half]
        outs[1][rows, :] = value[:, half:]

    def work():
        for index, (q_cols, k_cols, v_cols, rows, factor) in enumerate(MAPS):
            keys = jnp.concatenate([r[:, k_cols] for r in kv_refs], axis=0)
            queries = jnp.concatenate([own_q_ref[:, q_cols], got_q_ref[:, q_cols]], axis=0)
            values = jnp.concatenate([r[:, v_cols] for r in kv_refs], axis=0)
            scores = (
                lax.dot_general(
                    keys,
                    queries,
                    (((1,), (1,)), ((), ())),
                    preferred_element_type=jnp.float32,
                )
                * factor
            )
            at_max = slice(SUMS + index, SUMS + index + 1)
            at_sum = slice(SUMS + 4 + index, SUMS + 5 + index)
            if first:
                key_seg = lax.broadcasted_iota(jnp.int32, scores.shape, 0) // SEG
                column = lax.broadcasted_iota(jnp.int32, scores.shape, 1)
                query_seg = jnp.where(
                    column < half, column // SEG, (column - half) // SEG + flag_ref[0]
                )
                visible = key_seg <= query_seg
                scores = jnp.where(visible, scores, LOW)
                new_max = jnp.max(scores, axis=0, keepdims=True)
                expo = jnp.where(visible, jnp.exp(scores - new_max), 0.0)
            else:
                old_max = both(olds, at_max)
                new_max = jnp.maximum(old_max, jnp.max(scores, axis=0, keepdims=True))
                expo = jnp.exp(scores - new_max)
            total = jnp.sum(expo, axis=0, keepdims=True)
            summed = lax.dot_general(
                values,
                expo.astype(jnp.bfloat16),
                (((0,), (0,)), ((), ())),
                preferred_element_type=jnp.float32,
            )
            if not first:
                shrink = jnp.exp(old_max - new_max)
                total = total + both(olds, at_sum) * shrink
                summed = summed + both(olds, rows) * shrink
            keep(rows, summed)
            keep(at_max, new_max)
            keep(at_sum, total)

    if first:
        work()
    else:
        pl.when(flag_ref[0] > 0)(work)

        @pl.when(flag_ref[0] <= 0)
        def _():
            outs[0][...] = olds[0][...]
            outs[1][...] = olds[1][...]


def absorbed(flag, queries, kvs, olds):
    half = queries[0].shape[0]
    shape = jax.ShapeDtypeStruct((STATE, half), jnp.float32)
    keys = len(kvs) * kvs[0].shape[0]
    return pl.pallas_call(
        functools.partial(absorb, olds is None, len(kvs)),
        out_shape=(shape, shape),
        in_specs=[SMEM] + [VMEM] * (2 + len(kvs) + (0 if olds is None else 2)),
        out_specs=(VMEM, VMEM),
        cost_estimate=pl.CostEstimate(
            flops=2 * 2 * half * keys * (512 + SUMS), bytes_accessed=0, transcendentals=0
        ),
        compiler_params=pltpu.CompilerParams(vmem_limit_bytes=12 << 20),
        name="absorb",
    )(flag, *queries, *kvs, *(olds or ()))


def pack(qa_ref, qb_ref, ka_ref, va_ref, kb_ref, vb_ref, gate_ref, up_ref, down_ref, *refs):
    q_ref, kv_ref, out_ref, qa_buf, buf, sems = refs
    width = qa_buf.shape[1]
    q_cols = q_ref.shape[1] - kv_ref.shape[1]
    deep, wide = gate_ref.shape
    count = 0

    def begin(places):
        nonlocal count
        copies = []
        for a, b in places:
            copies.append(pltpu.make_async_copy(a, b, sems.at[count]))
            copies[-1].start()
            count += 1
        return copies

    first = begin(
        (
            (qa_ref, qa_buf),
            (ka_ref, kv_ref.at[:, :width]),
            (va_ref, kv_ref.at[:, width : 2 * width]),
            (kb_ref, kv_ref.at[:, 2 * width : 4 * width]),
            (vb_ref, kv_ref.at[:, 4 * width :]),
            (qb_ref, q_ref.at[:, 2 * width : q_cols]),
        )
    )
    pieces = []
    chunk = deep // 2
    for start in range(0, deep, chunk):
        rows = slice(start, start + chunk)
        sides = ((gate_ref, slice(0, wide)), (up_ref, slice(wide, 2 * wide)))
        pieces.append((rows, begin([(ref.at[rows, :], buf.at[rows, cols]) for ref, cols in sides])))
    places = []
    for j in range(deep // (2 * wide)):
        start = deep + j * wide
        cols = slice(2 * j * wide, 2 * (j + 1) * wide)
        places.append((down_ref.at[:, cols], buf.at[start : start + wide, :]))
    pieces.append((slice(deep, deep + deep // 2), begin(places)))
    for copy in first:
        copy.wait()
    both = qa_buf[...]
    first_map = lax.broadcasted_iota(jnp.int32, both.shape, 1) < DK_A
    q_ref[:, :width] = jnp.where(first_map, both, 0)
    q_ref[:, width : 2 * width] = jnp.where(first_map, 0, both)
    q_ref[:, q_cols:] = kv_ref[...]
    outs = []
    for rows, copies in pieces:
        for copy in copies:
            copy.wait()
        outs += begin([(buf.at[rows, :], out_ref.at[rows, :])])
    for copy in outs:
        copy.wait()


def fetch(*refs):
    count = (len(refs) - 1) // 2
    sems = refs[-1]
    copies = [pltpu.make_async_copy(refs[i], refs[count + i], sems.at[i]) for i in range(count)]
    for copy in copies:
        copy.start()
    for copy in copies:
        copy.wait()


def finish(mix_ref, at_ref, own_ref, got_ref, *refs):
    gain_a_ref, gain_b_ref, proj_a_ref, proj_b_ref, residual_ref, out_ref, cols_ref, sem = refs
    start = pl.multiple_of(at_ref[0] * cols_ref.shape[1], cols_ref.shape[1])
    copy = pltpu.make_async_copy(
        residual_ref.at[:, pl.ds(start, cols_ref.shape[1])], cols_ref, sem
    )
    copy.start()

    def merged(index):
        at_max = slice(SUMS + index, SUMS + index + 1)
        at_sum = slice(SUMS + 4 + index, SUMS + 5 + index)
        rows = MAPS[index][3]
        own_max, got_max = own_ref[at_max, :], got_ref[at_max, :]
        new_max = jnp.maximum(own_max, got_max)
        own_w, got_w = jnp.exp(own_max - new_max), jnp.exp(got_max - new_max)
        total = own_ref[at_sum, :] * own_w + got_ref[at_sum, :] * got_w
        return own_ref[rows, :] * (own_w / total) + got_ref[rows, :] * (got_w / total)

    def head(index, mixing, gain_ref):
        mixed = merged(index) - mixing * merged(index + 1)
        mean_sq = jnp.mean(mixed * mixed, axis=0, keepdims=True)
        gain = jnp.broadcast_to(gain_ref[...], mixed.shape[::-1]).T
        return (mixed * lax.rsqrt(mean_sq + EPS) * gain).astype(jnp.bfloat16)

    heads_a = head(0, mix_ref[0], gain_a_ref)
    heads_b = head(2, mix_ref[1], gain_b_ref)
    width = out_ref.shape[2]
    across = (((0,), (0,)), ((), ()))
    step = 4
    for piece in range(0, out_ref.shape[0], step):
        cols = slice(piece * width, (piece + step) * width)
        branch = lax.dot_general(
            heads_a, proj_a_ref[:, cols], across, preferred_element_type=jnp.float32
        ) + lax.dot_general(
            heads_b, proj_b_ref[:, cols], across, preferred_element_type=jnp.float32
        )
        for i in range(step):
            out_ref[piece + i] = branch[:, i * width : (i + 1) * width].astype(jnp.bfloat16)
    copy.wait()


def place(arrived_ref, residual_ref, select_ref, stream_ref, send_ref):
    summed = arrived_ref[0].astype(jnp.float32)
    for i in range(1, arrived_ref.shape[0]):
        summed = summed + arrived_ref[i].astype(jnp.float32)
    stream = (residual_ref[...].astype(jnp.float32) + summed).astype(jnp.bfloat16)
    stream_ref[...] = stream
    send_ref[...] = lax.dot_general(
        select_ref[...], stream, (((0,), (0,)), ((), ())), preferred_element_type=jnp.float32
    ).astype(jnp.bfloat16)


def experts(rows_ref, gain_ref, *refs):
    here, froms, out_ref, bufs, sems = refs[0], refs[1:LINE], refs[LINE], refs[LINE + 1 : -1], refs[-1]
    copies = [pltpu.make_async_copy(a, b, sems.at[i]) for i, (a, b) in enumerate(zip(froms, bufs))]
    for copy in copies:
        copy.start()
    parts, group_rows, width = rows_ref.shape
    parts = parts // 2
    model_width = parts * width
    rows = jnp.concatenate(
        [
            jnp.concatenate([rows_ref[core * parts + i] for i in range(parts)], axis=1)
            for core in range(2)
        ],
        axis=0,
    ).astype(jnp.float32)
    mean_sq = jnp.sum(rows * rows, axis=1, keepdims=True) / model_width
    normed = (rows * lax.rsqrt(mean_sq + EPS) * gain_ref[...]).astype(jnp.bfloat16)

    def dot(a, b):
        return jnp.dot(a, b, preferred_element_type=jnp.float32)

    hidden = []
    bufs = (here, *bufs)
    for index, ref in enumerate(bufs):
        if index > 0:
            copies[index - 1].wait()
        both = dot(normed, ref[:model_width, :])
        gate, up = both[:, :width], both[:, width:]
        hidden.append((gate / (1.0 + jnp.exp(-gate)) * up).astype(jnp.bfloat16))
    for j in range(parts // 2):
        start = model_width + j * width
        down = dot(hidden[0], bufs[0][start : start + width, :])
        for i in range(1, LINE):
            down = down + dot(hidden[i], bufs[i][start : start + width, :])
        down = down.astype(jnp.bfloat16)
        for core in range(2):
            half = down[core * group_rows : (core + 1) * group_rows]
            out_ref[core * parts + 2 * j] = half[:, :width]
            out_ref[core * parts + 2 * j + 1] = half[:, width:]


def held(value):
    return pltpu.with_memory_space_constraint(value, pltpu.HBM)


def summed_on_arrival(pieces, axis):
    arrived = lax.all_to_all(pieces, axis, split_axis=0, concat_axis=0, tiled=True)
    return arrived.astype(jnp.float32)


def local(
    residual,
    query_a,
    keys_a,
    values_a,
    query_b,
    keys_b,
    values_b,
    lambda_a,
    lambda_b,
    gain_a,
    gain_b,
    proj_a,
    proj_b,
    norm_gain,
    routes,
    route_weight,
    expert_gate,
    expert_up,
    expert_down,
):
    tok_rows = residual.shape[0]
    model_width = residual.shape[1]
    seq_devices = lax.axis_size("z") * lax.axis_size("core")
    head_devices = lax.axis_size("tp")
    head_index = lax.axis_index("tp")
    seq_index = lax.axis_index(SEQ)
    columns = model_width // head_devices

    chips = seq_devices // 2
    chip, core = seq_index // 2, seq_index % 2
    partner = [(i, i ^ 1) for i in range(seq_devices)]
    half_way = chips // 2

    quarter = half_way // 2

    def onward(step, up_blocks, down_blocks):
        up = [block + step for block in up_blocks if block + step < chips]
        down = [(block - step) % chips for block in down_blocks]
        return [(2 * i - 1, 2 * i + 1) for i in up] + [(2 * ((i + 1) % chips), 2 * i) for i in down]

    fields = [a[:, 0] for a in (query_a, query_b, keys_a, values_a, keys_b, values_b)]
    deep, width = expert_gate.shape[1:]
    weights = [a[0] for a in (expert_gate, expert_up, expert_down)]
    own_all, own_kv, packed = pl.pallas_call(
        pack,
        out_shape=(
            jax.ShapeDtypeStruct((tok_rows, 4 * DK_B + SUMS), jnp.bfloat16),
            jax.ShapeDtypeStruct((tok_rows, SUMS), jnp.bfloat16),
            pltpu.HBM((deep + deep // 2, 2 * width), jnp.bfloat16),
        ),
        in_specs=[HBM] * 9,
        out_specs=(VMEM, VMEM, HBM),
        scratch_shapes=[
            pltpu.VMEM(fields[0].shape, jnp.bfloat16),
            pltpu.VMEM((deep + deep // 2, 2 * width), jnp.bfloat16),
            pltpu.SemaphoreType.DMA((6 + 4 + deep // (2 * width) + 3,)),
        ],
        compiler_params=pltpu.CompilerParams(vmem_limit_bytes=8 << 20),
        name="pack",
    )(*[held(a) for a in fields + weights])
    got_all = lax.ppermute(own_all, SEQ, partner)
    got_kv = got_all[:, 4 * DK_B :]
    queries = (own_all, got_all)

    lines = head_devices // LINE
    packed = [packed]
    along = [
        (s * head_devices + t, s * head_devices + (t + (lines if s % 2 == 0 else -lines)) % head_devices)
        for s in range(seq_devices)
        for t in range(head_devices)
    ]
    for _ in range(1, LINE):
        packed.append(lax.ppermute(packed[-1], (*SEQ, "tp"), along))

    segments = tok_rows // SEG
    later = jnp.where(core == 0, segments, -segments).astype(jnp.int32).reshape(1)
    state = absorbed(later, queries, (own_kv,), None)
    mine, theirs = own_kv, got_kv
    for step in range(1, half_way):
        source = jnp.where(core == 1, chip - step, chip + step) % chips
        seen = (source < chip).astype(jnp.int32).reshape(1)
        pairs = onward(step, range(chips), range(half_way - 1))
        mine = lax.ppermute(mine, SEQ, pairs)
        theirs = lax.ppermute(theirs, SEQ, pairs)
        state = absorbed(seen, queries, (mine, theirs), state)
    near = (chip >= half_way) & (chip < half_way + quarter)
    mine = lax.ppermute(mine, SEQ, onward(half_way, range(half_way), range(quarter)))
    theirs = lax.ppermute(theirs, SEQ, onward(half_way, range(quarter, half_way), ()))
    seen = jnp.where(core == 1, chip >= half_way, near).astype(jnp.int32).reshape(1)
    state = absorbed(seen, queries, (mine,), state)
    seen = ((core == 1) & (chip >= half_way + quarter)).astype(jnp.int32).reshape(1)
    state = absorbed(seen, queries, (theirs,), state)
    got_state = lax.ppermute(state[1], SEQ, partner)
    projs = pl.pallas_call(
        fetch,
        out_shape=tuple(pltpu.VMEM(a.shape, jnp.bfloat16) for a in (proj_a, proj_b)),
        in_specs=[HBM] * 2,
        out_specs=(VMEM, VMEM),
        scratch_shapes=[pltpu.SemaphoreType.DMA((2,))],
        compiler_params=pltpu.CompilerParams(vmem_limit_bytes=4 << 20),
        name="fetch",
    )(held(proj_a), held(proj_b))
    mix = jnp.concatenate([lambda_a, lambda_b])
    pieces, residual_cols = pl.pallas_call(
        finish,
        out_shape=(
            jax.ShapeDtypeStruct((head_devices, tok_rows, columns), jnp.bfloat16),
            jax.ShapeDtypeStruct((tok_rows, columns), jnp.bfloat16),
        ),
        in_specs=[SMEM] * 2 + [VMEM] * 6 + [HBM],
        out_specs=(VMEM, VMEM),
        scratch_shapes=[pltpu.SemaphoreType.DMA],
        cost_estimate=pl.CostEstimate(
            flops=2 * tok_rows * model_width * 384, bytes_accessed=0, transcendentals=0
        ),
        compiler_params=pltpu.CompilerParams(vmem_limit_bytes=16 << 20),
        name="finish",
    )(
        mix,
        head_index.astype(jnp.int32).reshape(1),
        state[0],
        got_state,
        gain_a[None, :],
        gain_b[None, :],
        *projs,
        held(residual),
    )

    arrived = lax.all_to_all(pieces, "tp", split_axis=0, concat_axis=0, tiled=True)
    slot_count = 2 * tok_rows * TOP // seq_devices
    assign = routes.reshape(-1)
    onehot = (assign[:, None] == jnp.arange(seq_devices, dtype=jnp.int32)[None, :]).astype(
        jnp.int32
    )
    earlier = jnp.cumsum(onehot, axis=0) - onehot
    slot_index = jnp.sum(earlier * onehot, axis=1)
    target = assign * slot_count + slot_index
    placed = (
        target[:, None] == jnp.arange(seq_devices * slot_count, dtype=jnp.int32)[None, :]
    ).reshape(tok_rows, TOP, -1)
    select = jnp.sum(placed.astype(jnp.bfloat16), axis=1)
    gates = route_weight / jnp.sum(route_weight, axis=1, keepdims=True)
    combine = jnp.sum(placed.astype(jnp.float32) * gates[:, :, None], axis=1)
    stream_cols, send_rows = pl.pallas_call(
        place,
        out_shape=(
            jax.ShapeDtypeStruct((tok_rows, columns), jnp.bfloat16),
            jax.ShapeDtypeStruct((seq_devices * slot_count, columns), jnp.bfloat16),
        ),
        in_specs=[VMEM] * 3,
        out_specs=(VMEM, VMEM),
        compiler_params=pltpu.CompilerParams(vmem_limit_bytes=4 << 20),
        name="place",
    )(arrived, residual_cols, select)
    routed = lax.all_to_all(
        send_rows.reshape(chips, 2 * slot_count, columns),
        "z",
        split_axis=0,
        concat_axis=0,
        tiled=True,
    )
    share = chips // LINE
    group_rows = share * slot_count
    grouped = routed.reshape(LINE, share, 2, slot_count, columns).transpose(2, 0, 1, 3, 4)
    copies = jnp.broadcast_to(
        grouped.reshape(2, LINE, 1, group_rows, columns), (2, LINE, lines, group_rows, columns)
    )
    arrived = lax.all_to_all(
        copies.reshape(2 * head_devices, group_rows, columns),
        ("core", "tp"),
        split_axis=0,
        concat_axis=0,
        tiled=True,
    )
    parts = pl.pallas_call(
        experts,
        out_shape=jax.ShapeDtypeStruct((2 * head_devices, group_rows, columns), jnp.bfloat16),
        in_specs=[VMEM] * 3 + [HBM] * (LINE - 1),
        out_specs=VMEM,
        scratch_shapes=[
            pltpu.VMEM(packed[0].shape, jnp.bfloat16) for _ in range(LINE - 1)
        ]
        + [pltpu.SemaphoreType.DMA((LINE - 1,))],
        cost_estimate=pl.CostEstimate(
            flops=12 * group_rows * model_width * LINE * width, bytes_accessed=0, transcendentals=0
        ),
        compiler_params=pltpu.CompilerParams(vmem_limit_bytes=24 << 20),
        name="experts",
    )(arrived, norm_gain[None, :], packed[-1], *[held(a) for a in packed[:-1]])
    results = (
        summed_on_arrival(parts, ("core", "tp"))
        .reshape(2, LINE, lines, share, slot_count, columns)
        .sum(axis=2)
        .astype(jnp.bfloat16)
        .transpose(1, 2, 0, 3, 4)
        .reshape(chips, 2 * slot_count, columns)
    )
    returned = lax.all_to_all(results, "z", split_axis=0, concat_axis=0, tiled=True)
    returned_flat = returned.reshape(seq_devices * slot_count, columns).astype(jnp.float32)
    experts_sum = jnp.dot(combine, returned_flat, precision=lax.Precision.HIGHEST)
    return (stream_cols.astype(jnp.float32) + experts_sum).astype(jnp.bfloat16)


def solution(mesh):
    placed = (
        P(SEQ, None),
        P(SEQ, "tp", None),
        P(SEQ, "tp", None),
        P(SEQ, "tp", None),
        P(SEQ, "tp", None),
        P(SEQ, "tp", None),
        P(SEQ, "tp", None),
        P("tp"),
        P("tp"),
        P(),
        P(),
        P("tp", None),
        P("tp", None),
        P(),
        P(SEQ, None),
        P(SEQ, None),
        P(SEQ, None, "tp"),
        P(SEQ, None, "tp"),
        P(SEQ, "tp", None),
    )
    split = Mesh(mesh.devices.reshape(-1, 2, mesh.shape["tp"]), (*SEQ, "tp"))
    return jax.shard_map(
        local, mesh=split, in_specs=placed, out_specs=P(SEQ, "tp"), check_vma=False
    )
```

```python
import functools

import jax
import jax.numpy as jnp
from jax import lax
from jax.experimental import pallas as pl
from jax.experimental.pallas import tpu as pltpu
from jax.sharding import Mesh
from jax.sharding import PartitionSpec as P


DK_A = 64
DK_B = 128
SEG = 64
TOP = 2
LINE = 4
EPS = 1e-06
LOW = -1e30


VMEM = pl.BlockSpec(memory_space=pltpu.VMEM)
SMEM = pl.BlockSpec(memory_space=pltpu.SMEM)
HBM = pl.BlockSpec(memory_space=pltpu.HBM)

MAPS = (
    (slice(0, 128), slice(0, 128), slice(128, 256), slice(0, 128), DK_A**-0.5),
    (slice(128, 256), slice(0, 128), slice(128, 256), slice(128, 256), DK_A**-0.5),
    (slice(256, 384), slice(256, 384), slice(512, 768), slice(256, 512), DK_B**-0.5),
    (slice(384, 512), slice(384, 512), slice(512, 768), slice(512, 768), DK_B**-0.5),
)
SUMS = 768
SEQ = ("z", "core")
STATE = SUMS + 8


def absorb(first, blocks, flag_ref, own_q_ref, got_q_ref, *refs):
    kv_refs = refs[:blocks]
    olds = None if first else refs[blocks : blocks + 2]
    outs = refs[-2:]
    half = outs[0].shape[1]

    def both(refs, rows):
        return jnp.concatenate([r[rows, :] for r in refs], axis=1)

    def keep(rows, value):
        outs[0][rows, :] = value[:, :half]
        outs[1][rows, :] = value[:, half:]

    def work():
        for index, (q_cols, k_cols, v_cols, rows, factor) in enumerate(MAPS):
            keys = jnp.concatenate([r[:, k_cols] for r in kv_refs], axis=0)
            queries = jnp.concatenate([own_q_ref[:, q_cols], got_q_ref[:, q_cols]], axis=0)
            values = jnp.concatenate([r[:, v_cols] for r in kv_refs], axis=0)
            scores = (
                lax.dot_general(
                    keys,
                    queries,
                    (((1,), (1,)), ((), ())),
                    preferred_element_type=jnp.float32,
                )
                * factor
            )
            at_max = slice(SUMS + index, SUMS + index + 1)
            at_sum = slice(SUMS + 4 + index, SUMS + 5 + index)
            if first:
                key_seg = lax.broadcasted_iota(jnp.int32, scores.shape, 0) // SEG
                column = lax.broadcasted_iota(jnp.int32, scores.shape, 1)
                query_seg = jnp.where(
                    column < half, column // SEG, (column - half) // SEG + flag_ref[0]
                )
                visible = key_seg <= query_seg
                scores = jnp.where(visible, scores, LOW)
                new_max = jnp.max(scores, axis=0, keepdims=True)
                expo = jnp.where(visible, jnp.exp(scores - new_max), 0.0)
            else:
                old_max = both(olds, at_max)
                new_max = jnp.maximum(old_max, jnp.max(scores, axis=0, keepdims=True))
                expo = jnp.exp(scores - new_max)
            total = jnp.sum(expo, axis=0, keepdims=True)
            summed = lax.dot_general(
                values,
                expo.astype(jnp.bfloat16),
                (((0,), (0,)), ((), ())),
                preferred_element_type=jnp.float32,
            )
            if not first:
                shrink = jnp.exp(old_max - new_max)
                total = total + both(olds, at_sum) * shrink
                summed = summed + both(olds, rows) * shrink
            keep(rows, summed)
            keep(at_max, new_max)
            keep(at_sum, total)

    if first:
        work()
    else:
        pl.when(flag_ref[0] > 0)(work)

        @pl.when(flag_ref[0] <= 0)
        def _():
            outs[0][...] = olds[0][...]
            outs[1][...] = olds[1][...]


def absorbed(flag, queries, kvs, olds):
    half = queries[0].shape[0]
    shape = jax.ShapeDtypeStruct((STATE, half), jnp.float32)
    keys = len(kvs) * kvs[0].shape[0]
    return pl.pallas_call(
        functools.partial(absorb, olds is None, len(kvs)),
        out_shape=(shape, shape),
        in_specs=[SMEM] + [VMEM] * (2 + len(kvs) + (0 if olds is None else 2)),
        out_specs=(VMEM, VMEM),
        cost_estimate=pl.CostEstimate(
            flops=2 * 2 * half * keys * (512 + SUMS), bytes_accessed=0, transcendentals=0
        ),
        compiler_params=pltpu.CompilerParams(vmem_limit_bytes=12 << 20),
        name="absorb",
    )(flag, *queries, *kvs, *(olds or ()))


def pack(qa_ref, qb_ref, ka_ref, va_ref, kb_ref, vb_ref, gate_ref, up_ref, down_ref, *refs):
    q_ref, kv_ref, out_ref, qa_buf, buf, sems = refs
    width = qa_buf.shape[1]
    q_cols = q_ref.shape[1] - kv_ref.shape[1]
    deep, wide = gate_ref.shape
    count = 0

    def begin(places):
        nonlocal count
        copies = []
        for a, b in places:
            copies.append(pltpu.make_async_copy(a, b, sems.at[count]))
            copies[-1].start()
            count += 1
        return copies

    first = begin(
        (
            (qa_ref, qa_buf),
            (ka_ref, kv_ref.at[:, :width]),
            (va_ref, kv_ref.at[:, width : 2 * width]),
            (kb_ref, kv_ref.at[:, 2 * width : 4 * width]),
            (vb_ref, kv_ref.at[:, 4 * width :]),
            (qb_ref, q_ref.at[:, 2 * width : q_cols]),
        )
    )
    pieces = []
    chunk = deep // 2
    for start in range(0, deep, chunk):
        rows = slice(start, start + chunk)
        sides = ((gate_ref, slice(0, wide)), (up_ref, slice(wide, 2 * wide)))
        pieces.append((rows, begin([(ref.at[rows, :], buf.at[rows, cols]) for ref, cols in sides])))
    places = []
    for j in range(deep // (2 * wide)):
        start = deep + j * wide
        cols = slice(2 * j * wide, 2 * (j + 1) * wide)
        places.append((down_ref.at[:, cols], buf.at[start : start + wide, :]))
    pieces.append((slice(deep, deep + deep // 2), begin(places)))
    for copy in first:
        copy.wait()
    both = qa_buf[...]
    first_map = lax.broadcasted_iota(jnp.int32, both.shape, 1) < DK_A
    q_ref[:, :width] = jnp.where(first_map, both, 0)
    q_ref[:, width : 2 * width] = jnp.where(first_map, 0, both)
    q_ref[:, q_cols:] = kv_ref[...]
    outs = []
    for rows, copies in pieces:
        for copy in copies:
            copy.wait()
        outs += begin([(buf.at[rows, :], out_ref.at[rows, :])])
    for copy in outs:
        copy.wait()


def fetch(*refs):
    count = (len(refs) - 1) // 2
    sems = refs[-1]
    copies = [pltpu.make_async_copy(refs[i], refs[count + i], sems.at[i]) for i in range(count)]
    for copy in copies:
        copy.start()
    for copy in copies:
        copy.wait()


def finish(mix_ref, at_ref, own_ref, got_ref, *refs):
    gain_a_ref, gain_b_ref, proj_a_ref, proj_b_ref, residual_ref, out_ref, cols_ref, sem = refs
    start = pl.multiple_of(at_ref[0] * cols_ref.shape[1], cols_ref.shape[1])
    copy = pltpu.make_async_copy(
        residual_ref.at[:, pl.ds(start, cols_ref.shape[1])], cols_ref, sem
    )
    copy.start()

    def merged(index):
        at_max = slice(SUMS + index, SUMS + index + 1)
        at_sum = slice(SUMS + 4 + index, SUMS + 5 + index)
        rows = MAPS[index][3]
        own_max, got_max = own_ref[at_max, :], got_ref[at_max, :]
        new_max = jnp.maximum(own_max, got_max)
        own_w, got_w = jnp.exp(own_max - new_max), jnp.exp(got_max - new_max)
        total = own_ref[at_sum, :] * own_w + got_ref[at_sum, :] * got_w
        return own_ref[rows, :] * (own_w / total) + got_ref[rows, :] * (got_w / total)

    def head(index, mixing, gain_ref):
        mixed = merged(index) - mixing * merged(index + 1)
        mean_sq = jnp.mean(mixed * mixed, axis=0, keepdims=True)
        gain = jnp.broadcast_to(gain_ref[...], mixed.shape[::-1]).T
        return (mixed * lax.rsqrt(mean_sq + EPS) * gain).astype(jnp.bfloat16)

    heads_a = head(0, mix_ref[0], gain_a_ref)
    heads_b = head(2, mix_ref[1], gain_b_ref)
    width = out_ref.shape[2]
    across = (((0,), (0,)), ((), ()))
    step = 4
    for piece in range(0, out_ref.shape[0], step):
        cols = slice(piece * width, (piece + step) * width)
        branch = lax.dot_general(
            heads_a, proj_a_ref[:, cols], across, preferred_element_type=jnp.float32
        ) + lax.dot_general(
            heads_b, proj_b_ref[:, cols], across, preferred_element_type=jnp.float32
        )
        for i in range(step):
            out_ref[piece + i] = branch[:, i * width : (i + 1) * width].astype(jnp.bfloat16)
    copy.wait()


def place(arrived_ref, residual_ref, select_ref, stream_ref, send_ref):
    summed = arrived_ref[0].astype(jnp.float32)
    for i in range(1, arrived_ref.shape[0]):
        summed = summed + arrived_ref[i].astype(jnp.float32)
    stream = (residual_ref[...].astype(jnp.float32) + summed).astype(jnp.bfloat16)
    stream_ref[...] = stream
    send_ref[...] = lax.dot_general(
        select_ref[...], stream, (((0,), (0,)), ((), ())), preferred_element_type=jnp.float32
    ).astype(jnp.bfloat16)


def experts(rows_ref, gain_ref, *refs):
    here, froms, out_ref, bufs, sems = refs[0], refs[1:LINE], refs[LINE], refs[LINE + 1 : -1], refs[-1]
    copies = [pltpu.make_async_copy(a, b, sems.at[i]) for i, (a, b) in enumerate(zip(froms, bufs))]
    for copy in copies:
        copy.start()
    parts, group_rows, width = rows_ref.shape
    parts = parts // 2
    model_width = parts * width
    rows = jnp.concatenate(
        [
            jnp.concatenate([rows_ref[core * parts + i] for i in range(parts)], axis=1)
            for core in range(2)
        ],
        axis=0,
    ).astype(jnp.float32)
    mean_sq = jnp.sum(rows * rows, axis=1, keepdims=True) / model_width
    normed = (rows * lax.rsqrt(mean_sq + EPS) * gain_ref[...]).astype(jnp.bfloat16)

    def dot(a, b):
        return jnp.dot(a, b, preferred_element_type=jnp.float32)

    hidden = []
    bufs = (here, *bufs)
    for index, ref in enumerate(bufs):
        if index > 0:
            copies[index - 1].wait()
        both = dot(normed, ref[:model_width, :])
        gate, up = both[:, :width], both[:, width:]
        hidden.append((gate / (1.0 + jnp.exp(-gate)) * up).astype(jnp.bfloat16))
    pairs = [jnp.concatenate(hidden[i : i + 2], axis=1) for i in range(0, LINE, 2)]
    for j in range(parts // 2):
        start = model_width + j * width
        down = jnp.zeros((2 * group_rows, 2 * width), jnp.float32)
        for i in range(0, LINE, 2):
            both = [ref[start : start + width, :] for ref in bufs[i : i + 2]]
            down = down + dot(pairs[i // 2], jnp.concatenate(both, axis=0))
        down = down.astype(jnp.bfloat16)
        for core in range(2):
            half = down[core * group_rows : (core + 1) * group_rows]
            out_ref[core * parts + 2 * j] = half[:, :width]
            out_ref[core * parts + 2 * j + 1] = half[:, width:]


def held(value):
    return pltpu.with_memory_space_constraint(value, pltpu.HBM)


def summed_on_arrival(pieces, axis):
    arrived = lax.all_to_all(pieces, axis, split_axis=0, concat_axis=0, tiled=True)
    return arrived.astype(jnp.float32)


def local(
    residual,
    query_a,
    keys_a,
    values_a,
    query_b,
    keys_b,
    values_b,
    lambda_a,
    lambda_b,
    gain_a,
    gain_b,
    proj_a,
    proj_b,
    norm_gain,
    routes,
    route_weight,
    expert_gate,
    expert_up,
    expert_down,
):
    tok_rows = residual.shape[0]
    model_width = residual.shape[1]
    seq_devices = lax.axis_size("z") * lax.axis_size("core")
    head_devices = lax.axis_size("tp")
    head_index = lax.axis_index("tp")
    seq_index = lax.axis_index(SEQ)
    columns = model_width // head_devices

    chips = seq_devices // 2
    chip, core = seq_index // 2, seq_index % 2
    partner = [(i, i ^ 1) for i in range(seq_devices)]
    half_way = chips // 2

    quarter = half_way // 2

    def onward(step, up_blocks, down_blocks):
        up = [block + step for block in up_blocks if block + step < chips]
        down = [(block - step) % chips for block in down_blocks]
        return [(2 * i - 1, 2 * i + 1) for i in up] + [(2 * ((i + 1) % chips), 2 * i) for i in down]

    fields = [a[:, 0] for a in (query_a, query_b, keys_a, values_a, keys_b, values_b)]
    deep, width = expert_gate.shape[1:]
    weights = [a[0] for a in (expert_gate, expert_up, expert_down)]
    own_all, own_kv, packed = pl.pallas_call(
        pack,
        out_shape=(
            jax.ShapeDtypeStruct((tok_rows, 4 * DK_B + SUMS), jnp.bfloat16),
            jax.ShapeDtypeStruct((tok_rows, SUMS), jnp.bfloat16),
            pltpu.HBM((deep + deep // 2, 2 * width), jnp.bfloat16),
        ),
        in_specs=[HBM] * 9,
        out_specs=(VMEM, VMEM, HBM),
        scratch_shapes=[
            pltpu.VMEM(fields[0].shape, jnp.bfloat16),
            pltpu.VMEM((deep + deep // 2, 2 * width), jnp.bfloat16),
            pltpu.SemaphoreType.DMA((6 + 4 + deep // (2 * width) + 3,)),
        ],
        compiler_params=pltpu.CompilerParams(vmem_limit_bytes=8 << 20),
        name="pack",
    )(*[held(a) for a in fields + weights])
    got_all = lax.ppermute(own_all, SEQ, partner)
    got_kv = got_all[:, 4 * DK_B :]
    queries = (own_all[:, : 4 * DK_B], got_all[:, : 4 * DK_B])

    lines = head_devices // LINE
    packed = [packed]
    along = [
        (s * head_devices + t, s * head_devices + (t + (lines if s % 2 == 0 else -lines)) % head_devices)
        for s in range(seq_devices)
        for t in range(head_devices)
    ]
    for _ in range(1, LINE):
        packed.append(lax.ppermute(packed[-1], (*SEQ, "tp"), along))

    segments = tok_rows // SEG
    later = jnp.where(core == 0, segments, -segments).astype(jnp.int32).reshape(1)
    state = absorbed(later, queries, (own_kv,), None)
    mine, theirs = own_kv, got_kv
    for step in range(1, half_way):
        source = jnp.where(core == 1, chip - step, chip + step) % chips
        seen = (source < chip).astype(jnp.int32).reshape(1)
        pairs = onward(step, range(chips), range(half_way - 1))
        mine = lax.ppermute(mine, SEQ, pairs)
        theirs = lax.ppermute(theirs, SEQ, pairs)
        state = absorbed(seen, queries, (mine, theirs), state)
    near = (chip >= half_way) & (chip < half_way + quarter)
    mine = lax.ppermute(mine, SEQ, onward(half_way, range(half_way), range(quarter)))
    theirs = lax.ppermute(theirs, SEQ, onward(half_way, range(quarter, half_way), ()))
    seen = jnp.where(core == 1, chip >= half_way, near).astype(jnp.int32).reshape(1)
    state = absorbed(seen, queries, (mine,), state)
    seen = ((core == 1) & (chip >= half_way + quarter)).astype(jnp.int32).reshape(1)
    state = absorbed(seen, queries, (theirs,), state)
    got_state = lax.ppermute(state[1], SEQ, partner)
    projs = pl.pallas_call(
        fetch,
        out_shape=tuple(pltpu.VMEM(a.shape, jnp.bfloat16) for a in (proj_a, proj_b)),
        in_specs=[HBM] * 2,
        out_specs=(VMEM, VMEM),
        scratch_shapes=[pltpu.SemaphoreType.DMA((2,))],
        compiler_params=pltpu.CompilerParams(vmem_limit_bytes=4 << 20),
        name="fetch",
    )(held(proj_a), held(proj_b))
    mix = jnp.concatenate([lambda_a, lambda_b])
    pieces, residual_cols = pl.pallas_call(
        finish,
        out_shape=(
            jax.ShapeDtypeStruct((head_devices, tok_rows, columns), jnp.bfloat16),
            jax.ShapeDtypeStruct((tok_rows, columns), jnp.bfloat16),
        ),
        in_specs=[SMEM] * 2 + [VMEM] * 6 + [HBM],
        out_specs=(VMEM, VMEM),
        scratch_shapes=[pltpu.SemaphoreType.DMA],
        cost_estimate=pl.CostEstimate(
            flops=2 * tok_rows * model_width * 384, bytes_accessed=0, transcendentals=0
        ),
        compiler_params=pltpu.CompilerParams(vmem_limit_bytes=16 << 20),
        name="finish",
    )(
        mix,
        head_index.astype(jnp.int32).reshape(1),
        state[0],
        got_state,
        gain_a[None, :],
        gain_b[None, :],
        *projs,
        held(residual),
    )

    arrived = lax.all_to_all(pieces, "tp", split_axis=0, concat_axis=0, tiled=True)
    slot_count = 2 * tok_rows * TOP // seq_devices
    assign = routes.reshape(-1)
    onehot = (assign[:, None] == jnp.arange(seq_devices, dtype=jnp.int32)[None, :]).astype(
        jnp.int32
    )
    earlier = jnp.cumsum(onehot, axis=0) - onehot
    slot_index = jnp.sum(earlier * onehot, axis=1)
    target = assign * slot_count + slot_index
    placed = (
        target[:, None] == jnp.arange(seq_devices * slot_count, dtype=jnp.int32)[None, :]
    ).reshape(tok_rows, TOP, -1)
    select = jnp.sum(placed.astype(jnp.bfloat16), axis=1)
    gates = route_weight / jnp.sum(route_weight, axis=1, keepdims=True)
    combine = jnp.sum(placed.astype(jnp.float32) * gates[:, :, None], axis=1)
    stream_cols, send_rows = pl.pallas_call(
        place,
        out_shape=(
            jax.ShapeDtypeStruct((tok_rows, columns), jnp.bfloat16),
            jax.ShapeDtypeStruct((seq_devices * slot_count, columns), jnp.bfloat16),
        ),
        in_specs=[VMEM] * 3,
        out_specs=(VMEM, VMEM),
        compiler_params=pltpu.CompilerParams(vmem_limit_bytes=4 << 20),
        name="place",
    )(arrived, residual_cols, select)
    routed = lax.all_to_all(
        send_rows.reshape(chips, 2 * slot_count, columns),
        "z",
        split_axis=0,
        concat_axis=0,
        tiled=True,
    )
    share = chips // LINE
    group_rows = share * slot_count
    grouped = routed.reshape(LINE, share, 2, slot_count, columns).transpose(2, 0, 1, 3, 4)
    copies = jnp.broadcast_to(
        grouped.reshape(2, LINE, 1, group_rows, columns), (2, LINE, lines, group_rows, columns)
    )
    arrived = lax.all_to_all(
        copies.reshape(2 * head_devices, group_rows, columns),
        ("core", "tp"),
        split_axis=0,
        concat_axis=0,
        tiled=True,
    )
    parts = pl.pallas_call(
        experts,
        out_shape=jax.ShapeDtypeStruct((2 * head_devices, group_rows, columns), jnp.bfloat16),
        in_specs=[VMEM] * 3 + [HBM] * (LINE - 1),
        out_specs=VMEM,
        scratch_shapes=[
            pltpu.VMEM(packed[0].shape, jnp.bfloat16) for _ in range(LINE - 1)
        ]
        + [pltpu.SemaphoreType.DMA((LINE - 1,))],
        cost_estimate=pl.CostEstimate(
            flops=12 * group_rows * model_width * LINE * width, bytes_accessed=0, transcendentals=0
        ),
        compiler_params=pltpu.CompilerParams(vmem_limit_bytes=24 << 20),
        name="experts",
    )(arrived, norm_gain[None, :], packed[-1], *[held(a) for a in packed[:-1]])
    results = (
        summed_on_arrival(parts, ("core", "tp"))
        .reshape(2, LINE, lines, share, slot_count, columns)
        .sum(axis=2)
        .astype(jnp.bfloat16)
        .transpose(1, 2, 0, 3, 4)
        .reshape(chips, 2 * slot_count, columns)
    )
    returned = lax.all_to_all(results, "z", split_axis=0, concat_axis=0, tiled=True)
    returned_flat = returned.reshape(seq_devices * slot_count, columns).astype(jnp.float32)
    experts_sum = jnp.dot(combine, returned_flat, precision=lax.Precision.HIGHEST)
    return (stream_cols.astype(jnp.float32) + experts_sum).astype(jnp.bfloat16)


def solution(mesh):
    placed = (
        P(SEQ, None),
        P(SEQ, "tp", None),
        P(SEQ, "tp", None),
        P(SEQ, "tp", None),
        P(SEQ, "tp", None),
        P(SEQ, "tp", None),
        P(SEQ, "tp", None),
        P("tp"),
        P("tp"),
        P(),
        P(),
        P("tp", None),
        P("tp", None),
        P(),
        P(SEQ, None),
        P(SEQ, None),
        P(SEQ, None, "tp"),
        P(SEQ, None, "tp"),
        P(SEQ, "tp", None),
    )
    split = Mesh(mesh.devices.reshape(-1, 2, mesh.shape["tp"]), (*SEQ, "tp"))
    return jax.shard_map(
        local, mesh=split, in_specs=placed, out_specs=P(SEQ, "tp"), check_vma=False
    )
```

```python
import functools

import jax
import jax.numpy as jnp
from jax import lax
from jax.experimental import pallas as pl
from jax.experimental.pallas import tpu as pltpu
from jax.sharding import Mesh
from jax.sharding import PartitionSpec as P


DK_A = 64
DK_B = 128
SEG = 64
TOP = 2
LINE = 4
EPS = 1e-06
LOW = -1e30


VMEM = pl.BlockSpec(memory_space=pltpu.VMEM)
SMEM = pl.BlockSpec(memory_space=pltpu.SMEM)
HBM = pl.BlockSpec(memory_space=pltpu.HBM)

MAPS = (
    (slice(0, 128), slice(0, 128), slice(128, 256), slice(0, 128), DK_A**-0.5),
    (slice(128, 256), slice(0, 128), slice(128, 256), slice(128, 256), DK_A**-0.5),
    (slice(256, 384), slice(256, 384), slice(512, 768), slice(256, 512), DK_B**-0.5),
    (slice(384, 512), slice(384, 512), slice(512, 768), slice(512, 768), DK_B**-0.5),
)
SUMS = 768
SEQ = ("z", "core")
STATE = SUMS + 8


def absorb(first, blocks, flag_ref, own_q_ref, got_q_ref, *refs):
    kv_refs = refs[:blocks]
    olds = None if first else refs[blocks : blocks + 2]
    outs = refs[-2:]
    half = outs[0].shape[1]

    def both(refs, rows):
        return jnp.concatenate([r[rows, :] for r in refs], axis=1)

    def keep(rows, value):
        outs[0][rows, :] = value[:, :half]
        outs[1][rows, :] = value[:, half:]

    def work():
        for index, (q_cols, k_cols, v_cols, rows, factor) in enumerate(MAPS):
            keys = jnp.concatenate([r[:, k_cols] for r in kv_refs], axis=0)
            queries = jnp.concatenate([own_q_ref[:, q_cols], got_q_ref[:, q_cols]], axis=0)
            values = jnp.concatenate([r[:, v_cols] for r in kv_refs], axis=0)
            scores = (
                lax.dot_general(
                    keys,
                    queries,
                    (((1,), (1,)), ((), ())),
                    preferred_element_type=jnp.float32,
                )
                * factor
            )
            at_max = slice(SUMS + index, SUMS + index + 1)
            at_sum = slice(SUMS + 4 + index, SUMS + 5 + index)
            if first:
                key_seg = lax.broadcasted_iota(jnp.int32, scores.shape, 0) // SEG
                column = lax.broadcasted_iota(jnp.int32, scores.shape, 1)
                query_seg = jnp.where(
                    column < half, column // SEG, (column - half) // SEG + flag_ref[0]
                )
                visible = key_seg <= query_seg
                scores = jnp.where(visible, scores, LOW)
                new_max = jnp.max(scores, axis=0, keepdims=True)
                expo = jnp.where(visible, jnp.exp(scores - new_max), 0.0)
            else:
                old_max = both(olds, at_max)
                new_max = jnp.maximum(old_max, jnp.max(scores, axis=0, keepdims=True))
                expo = jnp.exp(scores - new_max)
            total = jnp.sum(expo, axis=0, keepdims=True)
            summed = lax.dot_general(
                values,
                expo.astype(jnp.bfloat16),
                (((0,), (0,)), ((), ())),
                preferred_element_type=jnp.float32,
            )
            if not first:
                shrink = jnp.exp(old_max - new_max)
                total = total + both(olds, at_sum) * shrink
                summed = summed + both(olds, rows) * shrink
            keep(rows, summed)
            keep(at_max, new_max)
            keep(at_sum, total)

    if first:
        work()
    else:
        pl.when(flag_ref[0] > 0)(work)

        @pl.when(flag_ref[0] <= 0)
        def _():
            outs[0][...] = olds[0][...]
            outs[1][...] = olds[1][...]


def absorbed(flag, queries, kvs, olds):
    half = queries[0].shape[0]
    shape = jax.ShapeDtypeStruct((STATE, half), jnp.float32)
    keys = len(kvs) * kvs[0].shape[0]
    return pl.pallas_call(
        functools.partial(absorb, olds is None, len(kvs)),
        out_shape=(shape, shape),
        in_specs=[SMEM] + [VMEM] * (2 + len(kvs) + (0 if olds is None else 2)),
        out_specs=(VMEM, VMEM),
        cost_estimate=pl.CostEstimate(
            flops=2 * 2 * half * keys * (512 + SUMS), bytes_accessed=0, transcendentals=0
        ),
        compiler_params=pltpu.CompilerParams(vmem_limit_bytes=12 << 20),
        name="absorb",
    )(flag, *queries, *kvs, *(olds or ()))


def pack(qa_ref, qb_ref, ka_ref, va_ref, kb_ref, vb_ref, gate_ref, up_ref, down_ref, *refs):
    q_ref, kv_ref, out_ref, qa_buf, buf, sems = refs
    width = qa_buf.shape[1]
    q_cols = q_ref.shape[1] - kv_ref.shape[1]
    deep, wide = gate_ref.shape
    count = 0

    def begin(places):
        nonlocal count
        copies = []
        for a, b in places:
            copies.append(pltpu.make_async_copy(a, b, sems.at[count]))
            copies[-1].start()
            count += 1
        return copies

    first = begin(
        (
            (qa_ref, qa_buf),
            (ka_ref, kv_ref.at[:, :width]),
            (va_ref, kv_ref.at[:, width : 2 * width]),
            (kb_ref, kv_ref.at[:, 2 * width : 4 * width]),
            (vb_ref, kv_ref.at[:, 4 * width :]),
            (qb_ref, q_ref.at[:, 2 * width : q_cols]),
        )
    )
    pieces = []
    chunk = deep // 2
    for start in range(0, deep, chunk):
        rows = slice(start, start + chunk)
        sides = ((gate_ref, slice(0, wide)), (up_ref, slice(wide, 2 * wide)))
        pieces.append((rows, begin([(ref.at[rows, :], buf.at[rows, cols]) for ref, cols in sides])))
    places = []
    for j in range(deep // (2 * wide)):
        start = deep + j * wide
        cols = slice(2 * j * wide, 2 * (j + 1) * wide)
        places.append((down_ref.at[:, cols], buf.at[start : start + wide, :]))
    pieces.append((slice(deep, deep + deep // 2), begin(places)))
    for copy in first:
        copy.wait()
    both = qa_buf[...]
    first_map = lax.broadcasted_iota(jnp.int32, both.shape, 1) < DK_A
    q_ref[:, :width] = jnp.where(first_map, both, 0)
    q_ref[:, width : 2 * width] = jnp.where(first_map, 0, both)
    q_ref[:, q_cols:] = kv_ref[...]
    outs = []
    for rows, copies in pieces:
        for copy in copies:
            copy.wait()
        outs += begin([(buf.at[rows, :], out_ref.at[rows, :])])
    for copy in outs:
        copy.wait()


def fetch(*refs):
    count = (len(refs) - 1) // 2
    sems = refs[-1]
    copies = [pltpu.make_async_copy(refs[i], refs[count + i], sems.at[i]) for i in range(count)]
    for copy in copies:
        copy.start()
    for copy in copies:
        copy.wait()


def finish(mix_ref, at_ref, own_ref, got_ref, *refs):
    gain_a_ref, gain_b_ref, proj_a_ref, proj_b_ref, residual_ref, out_ref, cols_ref, sem = refs
    start = pl.multiple_of(at_ref[0] * cols_ref.shape[1], cols_ref.shape[1])
    copy = pltpu.make_async_copy(
        residual_ref.at[:, pl.ds(start, cols_ref.shape[1])], cols_ref, sem
    )
    copy.start()

    def merged(index):
        at_max = slice(SUMS + index, SUMS + index + 1)
        at_sum = slice(SUMS + 4 + index, SUMS + 5 + index)
        rows = MAPS[index][3]
        own_max, got_max = own_ref[at_max, :], got_ref[at_max, :]
        new_max = jnp.maximum(own_max, got_max)
        own_w, got_w = jnp.exp(own_max - new_max), jnp.exp(got_max - new_max)
        total = own_ref[at_sum, :] * own_w + got_ref[at_sum, :] * got_w
        return own_ref[rows, :] * (own_w / total) + got_ref[rows, :] * (got_w / total)

    def head(index, mixing, gain_ref):
        mixed = merged(index) - mixing * merged(index + 1)
        mean_sq = jnp.mean(mixed * mixed, axis=0, keepdims=True)
        gain = jnp.broadcast_to(gain_ref[...], mixed.shape[::-1]).T
        return (mixed * lax.rsqrt(mean_sq + EPS) * gain).astype(jnp.bfloat16)

    heads_a = head(0, mix_ref[0], gain_a_ref)
    heads_b = head(2, mix_ref[1], gain_b_ref)
    width = out_ref.shape[2]
    across = (((0,), (0,)), ((), ()))
    step = 4
    for piece in range(0, out_ref.shape[0], step):
        cols = slice(piece * width, (piece + step) * width)
        branch = lax.dot_general(
            heads_a, proj_a_ref[:, cols], across, preferred_element_type=jnp.float32
        ) + lax.dot_general(
            heads_b, proj_b_ref[:, cols], across, preferred_element_type=jnp.float32
        )
        for i in range(step):
            out_ref[piece + i] = branch[:, i * width : (i + 1) * width].astype(jnp.bfloat16)
    copy.wait()


def place(arrived_ref, residual_ref, select_ref, stream_ref, send_ref):
    summed = arrived_ref[0].astype(jnp.float32)
    for i in range(1, arrived_ref.shape[0]):
        summed = summed + arrived_ref[i].astype(jnp.float32)
    stream = (residual_ref[...].astype(jnp.float32) + summed).astype(jnp.bfloat16)
    stream_ref[...] = stream
    send_ref[...] = lax.dot_general(
        select_ref[...], stream, (((0,), (0,)), ((), ())), preferred_element_type=jnp.float32
    ).astype(jnp.bfloat16)


def settle(parts_ref, out_ref):
    lines = parts_ref.shape[0] // (2 * LINE)
    chips, both, _ = out_ref.shape
    slots, share = both // 2, chips // LINE
    for core in range(2):
        for row in range(LINE):
            at = (core * LINE + row) * lines
            total = parts_ref[at].astype(jnp.float32)
            for i in range(1, lines):
                total = total + parts_ref[at + i].astype(jnp.float32)
            total = total.astype(jnp.bfloat16)
            for i in range(share):
                out_ref[row * share + i, core * slots : (core + 1) * slots] = total[
                    i * slots : (i + 1) * slots
                ]


def experts(rows_ref, gain_ref, *refs):
    here, froms, out_ref, bufs, sems = refs[0], refs[1:LINE], refs[LINE], refs[LINE + 1 : -1], refs[-1]
    copies = [pltpu.make_async_copy(a, b, sems.at[i]) for i, (a, b) in enumerate(zip(froms, bufs))]
    for copy in copies:
        copy.start()
    parts, group_rows, width = rows_ref.shape
    parts = parts // 2
    model_width = parts * width
    rows = jnp.concatenate(
        [
            jnp.concatenate([rows_ref[core * parts + i] for i in range(parts)], axis=1)
            for core in range(2)
        ],
        axis=0,
    ).astype(jnp.float32)
    mean_sq = jnp.sum(rows * rows, axis=1, keepdims=True) / model_width
    normed = (rows * lax.rsqrt(mean_sq + EPS) * gain_ref[...]).astype(jnp.bfloat16)

    def dot(a, b):
        return jnp.dot(a, b, preferred_element_type=jnp.float32)

    hidden = []
    bufs = (here, *bufs)
    for index, ref in enumerate(bufs):
        if index > 0:
            copies[index - 1].wait()
        both = dot(normed, ref[:model_width, :])
        gate, up = both[:, :width], both[:, width:]
        hidden.append((gate / (1.0 + jnp.exp(-gate)) * up).astype(jnp.bfloat16))
    pairs = [jnp.concatenate(hidden[i : i + 2], axis=1) for i in range(0, LINE, 2)]
    for j in range(parts // 2):
        start = model_width + j * width
        down = jnp.zeros((2 * group_rows, 2 * width), jnp.float32)
        for i in range(0, LINE, 2):
            both = [ref[start : start + width, :] for ref in bufs[i : i + 2]]
            down = down + dot(pairs[i // 2], jnp.concatenate(both, axis=0))
        down = down.astype(jnp.bfloat16)
        for core in range(2):
            half = down[core * group_rows : (core + 1) * group_rows]
            out_ref[core * parts + 2 * j] = half[:, :width]
            out_ref[core * parts + 2 * j + 1] = half[:, width:]


def held(value):
    return pltpu.with_memory_space_constraint(value, pltpu.HBM)


def local(
    residual,
    query_a,
    keys_a,
    values_a,
    query_b,
    keys_b,
    values_b,
    lambda_a,
    lambda_b,
    gain_a,
    gain_b,
    proj_a,
    proj_b,
    norm_gain,
    routes,
    route_weight,
    expert_gate,
    expert_up,
    expert_down,
):
    tok_rows = residual.shape[0]
    model_width = residual.shape[1]
    seq_devices = lax.axis_size("z") * lax.axis_size("core")
    head_devices = lax.axis_size("tp")
    head_index = lax.axis_index("tp")
    seq_index = lax.axis_index(SEQ)
    columns = model_width // head_devices

    chips = seq_devices // 2
    chip, core = seq_index // 2, seq_index % 2
    partner = [(i, i ^ 1) for i in range(seq_devices)]
    half_way = chips // 2

    quarter = half_way // 2

    def onward(step, up_blocks, down_blocks):
        up = [block + step for block in up_blocks if block + step < chips]
        down = [(block - step) % chips for block in down_blocks]
        return [(2 * i - 1, 2 * i + 1) for i in up] + [(2 * ((i + 1) % chips), 2 * i) for i in down]

    fields = [a[:, 0] for a in (query_a, query_b, keys_a, values_a, keys_b, values_b)]
    deep, width = expert_gate.shape[1:]
    weights = [a[0] for a in (expert_gate, expert_up, expert_down)]
    own_all, own_kv, packed = pl.pallas_call(
        pack,
        out_shape=(
            jax.ShapeDtypeStruct((tok_rows, 4 * DK_B + SUMS), jnp.bfloat16),
            jax.ShapeDtypeStruct((tok_rows, SUMS), jnp.bfloat16),
            pltpu.HBM((deep + deep // 2, 2 * width), jnp.bfloat16),
        ),
        in_specs=[HBM] * 9,
        out_specs=(VMEM, VMEM, HBM),
        scratch_shapes=[
            pltpu.VMEM(fields[0].shape, jnp.bfloat16),
            pltpu.VMEM((deep + deep // 2, 2 * width), jnp.bfloat16),
            pltpu.SemaphoreType.DMA((6 + 4 + deep // (2 * width) + 3,)),
        ],
        compiler_params=pltpu.CompilerParams(vmem_limit_bytes=8 << 20),
        name="pack",
    )(*[held(a) for a in fields + weights])
    got_all = lax.ppermute(own_all, SEQ, partner)
    got_kv = got_all[:, 4 * DK_B :]
    queries = (own_all[:, : 4 * DK_B], got_all[:, : 4 * DK_B])

    lines = head_devices // LINE
    packed = [packed]
    along = [
        (s * head_devices + t, s * head_devices + (t + (lines if s % 2 == 0 else -lines)) % head_devices)
        for s in range(seq_devices)
        for t in range(head_devices)
    ]
    for _ in range(1, LINE):
        packed.append(lax.ppermute(packed[-1], (*SEQ, "tp"), along))

    segments = tok_rows // SEG
    later = jnp.where(core == 0, segments, -segments).astype(jnp.int32).reshape(1)
    state = absorbed(later, queries, (own_kv,), None)
    mine, theirs = own_kv, got_kv
    for step in range(1, half_way):
        source = jnp.where(core == 1, chip - step, chip + step) % chips
        seen = (source < chip).astype(jnp.int32).reshape(1)
        pairs = onward(step, range(chips), range(half_way - 1))
        mine = lax.ppermute(mine, SEQ, pairs)
        theirs = lax.ppermute(theirs, SEQ, pairs)
        state = absorbed(seen, queries, (mine, theirs), state)
    near = (chip >= half_way) & (chip < half_way + quarter)
    mine = lax.ppermute(mine, SEQ, onward(half_way, range(half_way), range(quarter)))
    theirs = lax.ppermute(theirs, SEQ, onward(half_way, range(quarter, half_way), ()))
    seen = jnp.where(core == 1, chip >= half_way, near).astype(jnp.int32).reshape(1)
    state = absorbed(seen, queries, (mine,), state)
    seen = ((core == 1) & (chip >= half_way + quarter)).astype(jnp.int32).reshape(1)
    state = absorbed(seen, queries, (theirs,), state)
    got_state = lax.ppermute(state[1], SEQ, partner)
    projs = pl.pallas_call(
        fetch,
        out_shape=tuple(pltpu.VMEM(a.shape, jnp.bfloat16) for a in (proj_a, proj_b)),
        in_specs=[HBM] * 2,
        out_specs=(VMEM, VMEM),
        scratch_shapes=[pltpu.SemaphoreType.DMA((2,))],
        compiler_params=pltpu.CompilerParams(vmem_limit_bytes=4 << 20),
        name="fetch",
    )(held(proj_a), held(proj_b))
    mix = jnp.concatenate([lambda_a, lambda_b])
    pieces, residual_cols = pl.pallas_call(
        finish,
        out_shape=(
            jax.ShapeDtypeStruct((head_devices, tok_rows, columns), jnp.bfloat16),
            jax.ShapeDtypeStruct((tok_rows, columns), jnp.bfloat16),
        ),
        in_specs=[SMEM] * 2 + [VMEM] * 6 + [HBM],
        out_specs=(VMEM, VMEM),
        scratch_shapes=[pltpu.SemaphoreType.DMA],
        cost_estimate=pl.CostEstimate(
            flops=2 * tok_rows * model_width * 384, bytes_accessed=0, transcendentals=0
        ),
        compiler_params=pltpu.CompilerParams(vmem_limit_bytes=16 << 20),
        name="finish",
    )(
        mix,
        head_index.astype(jnp.int32).reshape(1),
        state[0],
        got_state,
        gain_a[None, :],
        gain_b[None, :],
        *projs,
        held(residual),
    )

    arrived = lax.all_to_all(pieces, "tp", split_axis=0, concat_axis=0, tiled=True)
    slot_count = 2 * tok_rows * TOP // seq_devices
    assign = routes.reshape(-1)
    onehot = (assign[:, None] == jnp.arange(seq_devices, dtype=jnp.int32)[None, :]).astype(
        jnp.int32
    )
    earlier = jnp.cumsum(onehot, axis=0) - onehot
    slot_index = jnp.sum(earlier * onehot, axis=1)
    target = assign * slot_count + slot_index
    placed = (
        target[:, None] == jnp.arange(seq_devices * slot_count, dtype=jnp.int32)[None, :]
    ).reshape(tok_rows, TOP, -1)
    select = jnp.sum(placed.astype(jnp.bfloat16), axis=1)
    gates = route_weight / jnp.sum(route_weight, axis=1, keepdims=True)
    combine = jnp.sum(placed.astype(jnp.float32) * gates[:, :, None], axis=1)
    stream_cols, send_rows = pl.pallas_call(
        place,
        out_shape=(
            jax.ShapeDtypeStruct((tok_rows, columns), jnp.bfloat16),
            jax.ShapeDtypeStruct((seq_devices * slot_count, columns), jnp.bfloat16),
        ),
        in_specs=[VMEM] * 3,
        out_specs=(VMEM, VMEM),
        compiler_params=pltpu.CompilerParams(vmem_limit_bytes=4 << 20),
        name="place",
    )(arrived, residual_cols, select)
    routed = lax.all_to_all(
        send_rows.reshape(chips, 2 * slot_count, columns),
        "z",
        split_axis=0,
        concat_axis=0,
        tiled=True,
    )
    share = chips // LINE
    group_rows = share * slot_count
    grouped = routed.reshape(LINE, share, 2, slot_count, columns).transpose(2, 0, 1, 3, 4)
    copies = jnp.broadcast_to(
        grouped.reshape(2, LINE, 1, group_rows, columns), (2, LINE, lines, group_rows, columns)
    )
    arrived = lax.all_to_all(
        copies.reshape(2 * head_devices, group_rows, columns),
        ("core", "tp"),
        split_axis=0,
        concat_axis=0,
        tiled=True,
    )
    parts = pl.pallas_call(
        experts,
        out_shape=jax.ShapeDtypeStruct((2 * head_devices, group_rows, columns), jnp.bfloat16),
        in_specs=[VMEM] * 3 + [HBM] * (LINE - 1),
        out_specs=VMEM,
        scratch_shapes=[
            pltpu.VMEM(packed[0].shape, jnp.bfloat16) for _ in range(LINE - 1)
        ]
        + [pltpu.SemaphoreType.DMA((LINE - 1,))],
        cost_estimate=pl.CostEstimate(
            flops=12 * group_rows * model_width * LINE * width, bytes_accessed=0, transcendentals=0
        ),
        compiler_params=pltpu.CompilerParams(vmem_limit_bytes=24 << 20),
        name="experts",
    )(arrived, norm_gain[None, :], packed[-1], *[held(a) for a in packed[:-1]])
    results = pl.pallas_call(
        settle,
        out_shape=jax.ShapeDtypeStruct((chips, 2 * slot_count, columns), jnp.bfloat16),
        in_specs=[VMEM],
        out_specs=VMEM,
        compiler_params=pltpu.CompilerParams(vmem_limit_bytes=4 << 20),
        name="settle",
    )(lax.all_to_all(parts, ("core", "tp"), split_axis=0, concat_axis=0, tiled=True))
    returned = lax.all_to_all(results, "z", split_axis=0, concat_axis=0, tiled=True)
    returned_flat = returned.reshape(seq_devices * slot_count, columns).astype(jnp.float32)
    experts_sum = jnp.dot(combine, returned_flat, precision=lax.Precision.HIGHEST)
    return (stream_cols.astype(jnp.float32) + experts_sum).astype(jnp.bfloat16)


def solution(mesh):
    placed = (
        P(SEQ, None),
        P(SEQ, "tp", None),
        P(SEQ, "tp", None),
        P(SEQ, "tp", None),
        P(SEQ, "tp", None),
        P(SEQ, "tp", None),
        P(SEQ, "tp", None),
        P("tp"),
        P("tp"),
        P(),
        P(),
        P("tp", None),
        P("tp", None),
        P(),
        P(SEQ, None),
        P(SEQ, None),
        P(SEQ, None, "tp"),
        P(SEQ, None, "tp"),
        P(SEQ, "tp", None),
    )
    split = Mesh(mesh.devices.reshape(-1, 2, mesh.shape["tp"]), (*SEQ, "tp"))
    return jax.shard_map(
        local, mesh=split, in_specs=placed, out_specs=P(SEQ, "tp"), check_vma=False
    )
```
